128 devices in a mesh: sp: 16 (over z, y), dp: 8 (over x, core).
Axes of the slice: x: 4, y: 4, z: 4, core: 2. Of those that a mesh axis runs over, the one named last changes fastest.
Arguments:
- query: bfloat16 [8, 3072, 3072], P('dp', 'sp'), may hold values from -18 to 18
- latent: bfloat16 [8, 3072, 1024], P('dp', 'sp'), may hold values from -6 to 6
- rope_key: bfloat16 [8, 3072, 32], P('dp', 'sp'), may hold values from -5 to 5
- latent_norm_gain: float32 [1024], replicated, may hold values from 0.1 to 1.9
- key_up_matrix: bfloat16 [2048, 1024], P('dp'), may hold values from -0.1875 to 0.1875
- value_up_matrix: bfloat16 [2048, 1024], P('dp'), may hold values from -0.1875 to 0.1875
- out_grad: bfloat16 [8, 3072, 2048], P('dp', 'sp'), may hold values from -6 to 6
Outputs:
- query_grad: bfloat16 [8, 3072, 3072], P('dp', 'sp')
- latent_grad: float32 [8, 3072, 1024], P('dp', 'sp')
- rope_key_grad: float32 [8, 3072, 32], P('dp', 'sp')
- key_weight_grad: float32 [2048, 1024], P('dp')
- value_weight_grad: float32 [2048, 1024], P('dp')
- gain_grad: float32 [1024], replicated
The draws below stay inside these ranges and needn't reach their ends.
All inputs are finite; a program needn't handle non-finite values.
Results may differ from the reference program's by a relative error of at most 0.011.
Values may be sent and summed in bfloat16 or wider, within the bound.
A program may use at most 256 MiB of HBM per device.

```python
import jax
import jax.numpy as jnp
from jax import lax

ATTENTION_HEADS = 32
PLAIN_HEAD_WIDTH = 64
ROPE = 32
VALUE_HEAD_WIDTH = 64
LATENT_WIDTH = 1024
SPAN = 64
SEQUENCE_LENGTH = 3072
BATCH_SEQUENCES = 8


def draw_rope_key(key, part):
    own = jax.random.fold_in(key, 11)
    values = jnp.clip(jax.random.normal(own, (BATCH_SEQUENCES, SEQUENCE_LENGTH, ROPE), jnp.float32), -5.0, 5.0)
    return values.astype(jnp.bfloat16)


def draw_query(key, part):
    own = jax.random.fold_in(key, 23)
    shape = (BATCH_SEQUENCES, SEQUENCE_LENGTH, ATTENTION_HEADS, PLAIN_HEAD_WIDTH + ROPE)
    values = jnp.clip(jax.random.normal(own, shape, jnp.float32), -5.0, 5.0)
    return values.reshape(BATCH_SEQUENCES, SEQUENCE_LENGTH, ATTENTION_HEADS * (PLAIN_HEAD_WIDTH + ROPE)).astype(jnp.bfloat16)


def block_scale(own_key, shape, split, least, high):
    loudness, own = 1.0, jax.random.fold_in(own_key, 6)
    for axis_at, blocks in split:
        steps = jnp.exp(jax.random.uniform(jax.random.fold_in(own, axis_at), (blocks,), jnp.float32, least / len(split), high / len(split)))
        loudness = loudness * jnp.repeat(steps, shape[axis_at] // blocks).reshape([-1 if axis == axis_at else 1 for axis in range(len(shape))])
    return loudness


def centred(rng, dims, scale, reach, split=(), held_as=jnp.bfloat16):
    result = scale * jax.random.normal(rng, dims, jnp.float32)
    if split:
        result = result * block_scale(rng, dims, split, -0.22, 0.18)
    return jnp.clip(result, -reach, reach).astype(held_as)


def setup_inputs(seed: int = 0) -> dict:
    streams_of = jax.random.split(jax.random.key(seed), 8)
    query = draw_query(jax.random.fold_in(streams_of[7], 71), 0)
    latent = centred(streams_of[1], (BATCH_SEQUENCES, SEQUENCE_LENGTH, LATENT_WIDTH), 1.0, 6.0, ((0, 8), (1, 16)))
    rope_key = draw_rope_key(jax.random.fold_in(streams_of[7], 71), 0)
    latent_norm_gain = jnp.clip(1.0 + 0.18 * jax.random.normal(streams_of[3], (LATENT_WIDTH,), jnp.float32), 0.1, 1.9)
    key_up_matrix = centred(streams_of[4], (ATTENTION_HEADS * PLAIN_HEAD_WIDTH, LATENT_WIDTH), LATENT_WIDTH ** -0.5, 0.1875, ((0, 8),))
    value_up_matrix = centred(streams_of[5], (ATTENTION_HEADS * VALUE_HEAD_WIDTH, LATENT_WIDTH), LATENT_WIDTH ** -0.5, 0.1875, ((0, 8),))
    out_grad = centred(streams_of[6], (BATCH_SEQUENCES, SEQUENCE_LENGTH, ATTENTION_HEADS * VALUE_HEAD_WIDTH), 1.0, 6.0, ((0, 8), (1, 16)))
    return {"query": query, "latent": latent, "rope_key": rope_key, "latent_norm_gain": latent_norm_gain, "key_up_matrix": key_up_matrix, "value_up_matrix": value_up_matrix, "out_grad": out_grad}


eps = 1e-06
rope_base = 10000.0

def rotate(values, cosine, sine):
    half = values.shape[-1] // 2
    first = values[..., :half]
    second = values[..., half:]
    return jnp.concatenate([first * cosine - second * sine, second * cosine + first * sine], axis=-1)

def angles(length, width):
    inverse = 1.0 / rope_base ** (jnp.arange(0, width, 2, dtype=jnp.float32) / width)
    turned = jnp.arange(length, dtype=jnp.float32)[:, None] * inverse[None, :]
    return (jnp.cos(turned), jnp.sin(turned))

def reference(query, latent, rope_key, latent_norm_gain, key_up_matrix, value_up_matrix, out_grad):
    f32 = jnp.float32
    bf16 = jnp.bfloat16
    length = SEQUENCE_LENGTH
    width = PLAIN_HEAD_WIDTH + ROPE
    scale = width ** (-0.5)
    block = 512 if length % 512 == 0 else length
    cosine, sine = angles(length, ROPE)
    neg = jnp.finfo(f32).min

    def one_sequence(inputs):
        seq_query, seq_latent, seq_rope, seq_grad = inputs
        lat = seq_latent.astype(f32)
        inv_rms = lax.rsqrt(lax.optimization_barrier(jnp.mean(lat * lat, axis=-1, keepdims=True)) + eps)
        normed = lat * inv_rms
        nlat = (normed * latent_norm_gain).astype(bf16)
        key_nope = jnp.dot(nlat, key_up_matrix.T, preferred_element_type=f32).astype(bf16).reshape(length, ATTENTION_HEADS, PLAIN_HEAD_WIDTH)
        values = jnp.dot(nlat, value_up_matrix.T, preferred_element_type=f32).astype(bf16).reshape(length, ATTENTION_HEADS, VALUE_HEAD_WIDTH)
        heads_query = seq_query.reshape(length, ATTENTION_HEADS, width)
        q_nope = heads_query[:, :, :PLAIN_HEAD_WIDTH]
        q_rope = rotate(heads_query[:, :, PLAIN_HEAD_WIDTH:].astype(f32), cosine[:, None, :], sine[:, None, :]).astype(bf16)
        k_rope = rotate(seq_rope.astype(f32), cosine, sine).astype(bf16)
        d_out = seq_grad.reshape(length, ATTENTION_HEADS, VALUE_HEAD_WIDTH)
        dk_nope = jnp.zeros((length, ATTENTION_HEADS, PLAIN_HEAD_WIDTH), f32)
        dk_rope = jnp.zeros((length, ROPE), f32)
        d_vals = jnp.zeros((length, ATTENTION_HEADS, VALUE_HEAD_WIDTH), f32)
        dq_parts = []
        for begin in range(0, length, block):
            end = begin + block
            qn = q_nope[begin:end].astype(f32)
            qr = q_rope[begin:end].astype(f32)
            go = d_out[begin:end].astype(f32)
            kn = key_nope[:end].astype(f32)
            kr = k_rope[:end].astype(f32)
            vv = values[:end].astype(f32)
            scores = (jnp.einsum('qhd,khd->hqk', qn, kn) + jnp.einsum('qhd,kd->hqk', qr, kr)) * scale
            q_seg = jnp.arange(begin, end) // SPAN
            k_seg = jnp.arange(end) // SPAN
            allowed = k_seg[None, :] <= q_seg[:, None]
            scores = jnp.where(allowed[None], scores, neg)
            probs = jax.nn.softmax(scores, axis=-1)
            d_probs = jnp.einsum('qhd,khd->hqk', go, vv)
            d_scores = probs * (d_probs - lax.optimization_barrier(jnp.sum(probs * d_probs, axis=-1, keepdims=True)))
            ds_b = d_scores.astype(bf16).astype(f32)
            p_b = probs.astype(bf16).astype(f32)
            dq_n = jnp.einsum('hqk,khd->qhd', ds_b, kn) * scale
            dq_r = jnp.einsum('hqk,kd->qhd', ds_b, kr) * scale
            dq_r = rotate(dq_r, cosine[begin:end, None, :], -sine[begin:end, None, :])
            dq_parts.append(jnp.concatenate([dq_n, dq_r], axis=-1).astype(bf16))
            dk_nope = dk_nope.at[:end].add(jnp.einsum('hqk,qhd->khd', ds_b, qn) * scale)
            dk_rope = dk_rope.at[:end].add(jnp.einsum('hqk,qhd->kd', ds_b, qr) * scale)
            d_vals = d_vals.at[:end].add(jnp.einsum('hqk,qhd->khd', p_b, go))
        query_grad = jnp.concatenate(dq_parts, axis=0).reshape(length, ATTENTION_HEADS * width)
        rope_grad = rotate(dk_rope, cosine, -sine)
        dk_b = dk_nope.astype(bf16).reshape(length, ATTENTION_HEADS * PLAIN_HEAD_WIDTH)
        dv_b = d_vals.astype(bf16).reshape(length, ATTENTION_HEADS * VALUE_HEAD_WIDTH)
        d_nlat = jnp.dot(dk_b, key_up_matrix, preferred_element_type=f32) + jnp.dot(dv_b, value_up_matrix, preferred_element_type=f32)
        key_part = jnp.dot(dk_b.T, nlat, preferred_element_type=f32)
        value_part = jnp.dot(dv_b.T, nlat, preferred_element_type=f32)
        gain_part = lax.optimization_barrier(jnp.sum(d_nlat * normed, axis=0))
        scaled = d_nlat * latent_norm_gain
        latent_grad = inv_rms * (scaled - normed * lax.optimization_barrier(jnp.mean(scaled * normed, axis=-1, keepdims=True)))
        return (query_grad, latent_grad, rope_grad, key_part, value_part, gain_part)
    results = lax.map(one_sequence, (query, latent, rope_key, out_grad))
    query_grad, latent_grad, rope_grad, key_parts, value_parts, gain_parts = results
    return (query_grad, latent_grad, rope_grad, lax.optimization_barrier(jnp.sum(key_parts, axis=0)), lax.optimization_barrier(jnp.sum(value_parts, axis=0)), lax.optimization_barrier(jnp.sum(gain_parts, axis=0)))
```

```python
import functools

import jax
import jax.numpy as jnp
import numpy as np
from jax import lax
from jax.experimental import pallas as pl
from jax.experimental.pallas import tpu as pltpu
from jax.sharding import Mesh
from jax.sharding import PartitionSpec as P

ATTENTION_HEADS = 32
PLAIN_HEAD_WIDTH = 64
ROPE = 32
VALUE_HEAD_WIDTH = 64
SPAN = 64
LATENT = 1024
LENGTH = 3072
TOKENS = 192
DP = ("dp_0", "dp_1")
SP = ("sp_0", "sp_1")
SP_DP = ("sp_0", "sp_1", "dp_0", "dp_1")
SP_SIZE = 16
DP_SIZE = 8
BLOCK = 512
SCALE = (PLAIN_HEAD_WIDTH + ROPE) ** (-0.5)
LOG2E = 1.4426950408889634

eps = 1e-06
rope_base = 10000.0
f32 = jnp.float32
bf16 = jnp.bfloat16


def pack_tables():
    first = np.zeros((384 + 256 + 128, 512), np.float32)
    second = np.zeros((384 + 256 + 128, 256), np.float32)
    for t in range(2):
        q, d, r = 192 * t, 384 + 128 * t, 640
        for c in range(64):
            first[q + c, 256 * t + c] = 1
            first[d + c, 256 * t + 64 + c] = 1
            second[q + 96 + c, 128 * t + c] = 1
            second[d + 64 + c, 128 * t + 64 + c] = 1
        for c in range(32):
            first[q + 64 + c, 256 * t + 128 + c] = 1
            first[q + 160 + c, 256 * t + 160 + c] = 1
            first[r + c, 256 * t + 192 + c] = 1
    return first, second


def unpack_table():
    place = np.zeros((512, 384), np.float32)
    for t in range(2):
        for h in range(2):
            for c in range(96):
                place[256 * t + 128 * h + c, 192 * t + 96 * h + c] = 1
    return place


def rope_tables():
    swap = np.zeros((128, 128), np.float32)
    for g in range(3):
        for c in range(16):
            swap[32 * g + 16 + c, 32 * g + c] = -1
            swap[32 * g + c, 32 * g + 16 + c] = 1
    spread = np.zeros((128, 384), np.float32)
    for c in range(32):
        spread[c, c] = 1
        spread[32 + c, 128 + c] = 1
        spread[64 + c, 256 + c] = 1
    for c in range(16):
        spread[64 + 16 + c, 256 + 32 + c] = 1
        spread[64 + c, 256 + 32 + 16 + c] = -1
    return swap, spread


def pack_kernel(query, d_out, rope, first, second, out0, out1):
    both = jnp.concatenate([query[...], d_out[...], rope[...]], axis=1)
    one = jnp.dot(both, first[...], preferred_element_type=f32).astype(bf16)
    two = jnp.dot(both, second[...], preferred_element_type=f32).astype(bf16)
    for t in range(2):
        out0[t] = one[:, 256 * t : 256 * t + 256]
        out1[t] = two[:, 128 * t : 128 * t + 128]


def pack(query, d_out, rope):
    first, second = pack_tables()
    whole = lambda shape: pl.BlockSpec(shape, lambda j: (0, 0))
    return pl.pallas_call(
        pack_kernel,
        grid=(8,),
        in_specs=[
            pl.BlockSpec((TOKENS, 384), lambda j: (0, j)),
            pl.BlockSpec((TOKENS, 256), lambda j: (0, j)),
            whole((TOKENS, 128)),
            whole((768, 512)),
            whole((768, 256)),
        ],
        out_specs=[
            pl.BlockSpec((2, TOKENS, 256), lambda j: (j, 0, 0)),
            pl.BlockSpec((2, TOKENS, 128), lambda j: (j, 0, 0)),
        ],
        out_shape=[
            jax.ShapeDtypeStruct((SP_SIZE, TOKENS, 256), bf16),
            jax.ShapeDtypeStruct((SP_SIZE, TOKENS, 128), bf16),
        ],
        cost_estimate=pl.CostEstimate(
            flops=16 * 192 * 768 * 768, bytes_accessed=5_000_000, transcendentals=0
        ),
        name="pack",
    )(query, d_out, rope, jnp.asarray(first, bf16), jnp.asarray(second, bf16))


def dot_t(a, b):
    return lax.dot_general(a, b, (((1,), (1,)), ((), ())), preferred_element_type=f32)


def lanes(x, combine):
    parts = [x[:, k : k + 128] for k in range(0, x.shape[1], 128)]
    return functools.reduce(combine, parts)


def attention_kernel(a_ref, q2_ref, kv_ref, k2_ref, tab_ref, out_ref, s_ref, dp_ref, m_ref, l_ref, d_ref, dq_ref, acc_ref):
    step = pl.program_id(0)
    count = LENGTH // BLOCK
    i = count - 1 - step

    @pl.when(step == 0)
    def _():
        acc_ref[...] = jnp.zeros_like(acc_ref)

    rows = pl.ds(pl.multiple_of(i * BLOCK, BLOCK), BLOCK)
    a = a_ref[rows, :]
    q2 = q2_ref[rows, :]
    lane = lax.broadcasted_iota(jnp.int32, (BLOCK, 128), 1)
    nope = jnp.where(lane < 64, a, jnp.zeros_like(a))
    cot = jnp.where(lane < 64, jnp.zeros_like(a), a)
    query = jnp.concatenate([nope, q2], axis=1)
    a_t = a.T
    q2_t = q2.T
    left_k = jnp.concatenate([q2_t[0:32], a_t[0:64]], axis=0)
    left_v = a_t[64:128]

    def tile(j):
        return pl.ds(pl.multiple_of(j * BLOCK, BLOCK), BLOCK)

    def key(j):
        return jnp.concatenate([kv_ref[tile(j), :], k2_ref[tile(j), :]], axis=1)

    m_ref[...] = jnp.full_like(m_ref, -1e30)
    l_ref[...] = jnp.zeros_like(l_ref)
    d_ref[...] = jnp.zeros_like(d_ref)
    dq_ref[...] = jnp.zeros_like(dq_ref)

    def scores(j, masked):
        s = dot_t(query, key(j))
        if masked:
            r = lax.broadcasted_iota(jnp.int32, (BLOCK, BLOCK), 0) // SPAN
            c = lax.broadcasted_iota(jnp.int32, (BLOCK, BLOCK), 1) // SPAN
            s = jnp.where(c <= r, s, -1e30)
        s_ref[:, tile(j)] = s
        m_ref[...] = jnp.maximum(m_ref[...], lanes(s, jnp.maximum))

    @pl.loop(0, i)
    def _(j):
        scores(j, False)

    scores(i, True)
    m = jnp.max(m_ref[...], axis=1, keepdims=True)

    def weights(j):
        dp = dot_t(cot, kv_ref[tile(j), :])
        e = jnp.exp2((s_ref[:, tile(j)] - m) * (SCALE * LOG2E))
        l_ref[...] += lanes(e, jnp.add)
        d_ref[...] += lanes(e * dp, jnp.add)
        s_ref[:, tile(j)] = e
        dp_ref[:, tile(j)] = dp

    @pl.loop(0, i + 1)
    def _(j):
        weights(j)

    inverse = 1.0 / jnp.sum(l_ref[...], axis=1, keepdims=True)
    delta = jnp.sum(d_ref[...], axis=1, keepdims=True) * inverse

    @pl.loop(0, i + 1)
    def _(j):
        p = s_ref[:, tile(j)] * inverse
        ds = (p * (dp_ref[:, tile(j)] - delta)).astype(bf16)
        dq_ref[...] += jnp.dot(ds, key(j), preferred_element_type=f32)
        acc_ref[0:96, tile(j)] += jnp.dot(left_k, ds, preferred_element_type=f32)
        acc_ref[96:160, tile(j)] += jnp.dot(left_v, p.astype(bf16), preferred_element_type=f32)

    turned = dq_ref[:, 128:256] * tab_ref[...]
    turned = turned + pltpu.roll(turned, 96, 1)
    dq = jnp.where(lane < 64, dq_ref[:, 0:128], pltpu.roll(turned, 64, 1)) * SCALE
    done = acc_ref[:, rows]
    k_rope = done[0:32] * SCALE
    k_nope = done[32:96] * SCALE
    low = jnp.concatenate([jnp.zeros((96, BLOCK), f32), k_rope], axis=0).T
    out_ref[:, 0:128] = jnp.where(lane < 96, dq, low).astype(bf16)
    out_ref[:, 128:256] = jnp.concatenate([k_nope, done[96:160]], axis=0).T.astype(bf16)


def attention(a, q2, kv, k2, table):
    count = LENGTH // BLOCK
    whole = pl.BlockSpec((LENGTH, 128), lambda i: (0, 0))
    return pl.pallas_call(
        attention_kernel,
        grid=(count,),
        in_specs=[whole] * 4 + [pl.BlockSpec((BLOCK, 128), lambda i: (count - 1 - i, 0))],
        out_specs=pl.BlockSpec((BLOCK, 256), lambda i: (count - 1 - i, 0)),
        out_shape=jax.ShapeDtypeStruct((LENGTH, 256), bf16),
        scratch_shapes=[
            pltpu.VMEM((BLOCK, LENGTH), f32),
            pltpu.VMEM((BLOCK, LENGTH), f32),
            pltpu.VMEM((BLOCK, 128), f32),
            pltpu.VMEM((BLOCK, 128), f32),
            pltpu.VMEM((BLOCK, 128), f32),
            pltpu.VMEM((BLOCK, 256), f32),
            pltpu.VMEM((160, LENGTH), f32),
        ],
        compiler_params=pltpu.CompilerParams(
            dimension_semantics=("arbitrary",), vmem_limit_bytes=48 * 1024 * 1024
        ),
        cost_estimate=pl.CostEstimate(
            flops=12_000_000_000, bytes_accessed=8_000_000, transcendentals=5_000_000
        ),
        name="attention",
    )(a, q2, kv, k2, table)


def finish_kernel(ret0, ret1, w, place, latent, gain, query_grad, latent_grad, rope_sum, acc):
    step = pl.program_id(0)

    @pl.when(step == 0)
    def _():
        acc[...] = jnp.zeros_like(acc)
        rope_sum[...] = jnp.zeros_like(rope_sum)

    left = [ret[t, :, 0:128] for t in range(2) for ret in (ret0, ret1)]
    query_grad[...] = jnp.dot(
        jnp.concatenate(left, axis=1), place[...], preferred_element_type=f32
    ).astype(bf16)
    rope_sum[...] += sum(x.astype(f32) for x in left)
    total = acc[...]
    for t in range(2):
        right = jnp.concatenate([ret0[t, :, 128:256], ret1[t, :, 128:256]], axis=1)
        total += jnp.dot(right, w[t], preferred_element_type=f32)
    acc[...] = total

    @pl.when(step == pl.num_programs(0) - 1)
    def _():
        lat = latent[...].astype(f32)
        inverse = lax.rsqrt(jnp.mean(lat * lat, axis=1, keepdims=True) + eps)
        normed = lat * inverse
        scaled = acc[...] * gain[...]
        latent_grad[...] = inverse * (
            scaled - normed * jnp.mean(scaled * normed, axis=1, keepdims=True)
        )


def finish(ret0, ret1, w, latent, gain):
    fixed = lambda shape: pl.BlockSpec(shape, lambda j: (0,) * len(shape))
    return pl.pallas_call(
        finish_kernel,
        grid=(8,),
        in_specs=[
            pl.BlockSpec((2, TOKENS, 256), lambda j: (j, 0, 0)),
            pl.BlockSpec((2, TOKENS, 256), lambda j: (j, 0, 0)),
            pl.BlockSpec((2, 256, LATENT), lambda j: (j, 0, 0)),
            fixed((512, 384)),
            fixed((TOKENS, LATENT)),
            fixed((1, LATENT)),
        ],
        out_specs=[
            pl.BlockSpec((TOKENS, 384), lambda j: (0, j)),
            fixed((TOKENS, LATENT)),
            fixed((TOKENS, 128)),
        ],
        out_shape=[
            jax.ShapeDtypeStruct((TOKENS, 3072), bf16),
            jax.ShapeDtypeStruct((TOKENS, LATENT), f32),
            jax.ShapeDtypeStruct((TOKENS, 128), f32),
        ],
        scratch_shapes=[pltpu.VMEM((TOKENS, LATENT), f32)],
        compiler_params=pltpu.CompilerParams(dimension_semantics=("arbitrary",)),
        cost_estimate=pl.CostEstimate(
            flops=4_000_000_000, bytes_accessed=14_000_000, transcendentals=0
        ),
        name="finish",
    )(ret0, ret1, w, jnp.asarray(unpack_table(), bf16), latent, gain)


def rotate(values, cosine, sine):
    half = values.shape[-1] // 2
    first = values[..., :half]
    second = values[..., half:]
    return jnp.concatenate(
        [first * cosine - second * sine, second * cosine + first * sine], axis=-1
    )


def inverse_frequency(index):
    return 1.0 / rope_base ** (2.0 * index.astype(f32) / ROPE)


def to_heads():
    pairs = []
    for i in range(DP_SIZE):
        for n in range(DP_SIZE):
            for b in range(2):
                pairs.append(((8 * b + n) * DP_SIZE + i, (2 * i + b) * DP_SIZE + n))
    return pairs


def exchange(value):
    return lax.all_to_all(value, SP, split_axis=0, concat_axis=0, tiled=True)


def local(query, latent, rope_key, latent_norm_gain, key_up_matrix, value_up_matrix, out_grad):
    lat = latent[0].astype(f32)
    inv_rms = lax.rsqrt(jnp.mean(lat * lat, axis=-1, keepdims=True) + eps)
    nlat = (lat * inv_rms * latent_norm_gain).astype(bf16)
    nlat_full = lax.all_gather(nlat, SP, axis=0, tiled=True)

    shard = jnp.stack(
        [key_up_matrix.reshape(2, 2, 64, LATENT), value_up_matrix.reshape(2, 2, 64, LATENT)],
        axis=2,
    ).reshape(2, 256, LATENT)
    spot = lax.axis_index(SP)
    half = lax.dynamic_index_in_dim(shard, spot // 8, 0, keepdims=False)
    w_own = lax.ppermute(half, SP_DP, to_heads())

    rope_wide = jnp.pad(rope_key[0], ((0, 0), (0, 96)))
    sent0, sent1 = pack(query[0], out_grad[0], rope_wide)
    got0 = exchange(sent0).reshape(LENGTH, 256)

    column = jnp.arange(128)
    turned = jnp.arange(LENGTH, dtype=f32)[:, None] * inverse_frequency(column % 16)[None, :]
    cosine = jnp.cos(turned)
    sine = jnp.sin(turned)
    table = jnp.where(column < 32, cosine, jnp.where(column < 64, sine, 0.0))
    swap, spread = rope_tables()

    raw = got0[:, 128:256]
    swapped = jnp.dot(raw, jnp.asarray(swap, bf16), preferred_element_type=f32)
    rotated = (raw.astype(f32) * cosine + swapped * sine).astype(bf16)
    apart = jnp.dot(rotated, jnp.asarray(spread, bf16), preferred_element_type=f32).astype(bf16)
    q2_0, q2_1, k2 = apart[:, 0:128], apart[:, 128:256], apart[:, 256:384]

    kv = lax.dot_general(
        nlat_full, w_own, (((1,), (1,)), ((), ())), preferred_element_type=f32
    ).astype(bf16)

    shard_later, _ = lax.optimization_barrier((shard, nlat_full))
    w_whole = lax.all_gather(shard_later, DP, axis=0, tiled=True)

    grads0 = attention(got0[:, 0:128], q2_0, kv[:, 0:128], k2, table)
    ret0 = exchange(grads0.reshape(SP_SIZE, TOKENS, 256))
    got1 = exchange(sent1).reshape(LENGTH, 128)
    grads1 = attention(got1, q2_1, kv[:, 128:256], k2, table)
    ret1 = exchange(grads1.reshape(SP_SIZE, TOKENS, 256))

    parts = [
        lax.dot_general(
            g[:, 128:256], nlat_full, (((0,), (0,)), ((), ())), preferred_element_type=f32
        )
        for g in (grads0, grads1)
    ]
    d_w = jnp.concatenate(parts, axis=0)
    gain_part = jnp.sum(d_w * w_own.astype(f32), axis=0) / latent_norm_gain
    gain_grad = lax.psum(gain_part, SP_DP)

    pieces = d_w.reshape(2, 2, 4, 16, LATENT).transpose(0, 2, 1, 3, 4).reshape(DP_SIZE, 32, LATENT)
    piece = lax.all_to_all(pieces, DP, split_axis=0, concat_axis=0, tiled=True).sum(axis=0)
    moved = lax.ppermute(piece, SP_DP, [(b, a) for a, b in to_heads()])
    blocks = lax.all_gather(moved, SP, axis=0, tiled=False)

    query_grad, latent_grad, rope_sum = finish(
        ret0, ret1, w_whole, latent[0], latent_norm_gain[None]
    )
    position = (spot * TOKENS + jnp.arange(TOKENS)).astype(f32)
    angle = position[:, None] * inverse_frequency(jnp.arange(16))[None, :]
    rope_grad = rotate(rope_sum[:, 96:128], jnp.cos(angle), -jnp.sin(angle))
    return (
        query_grad[None],
        latent_grad[None],
        rope_grad[None],
        blocks[:, 0:16].reshape(256, LATENT),
        blocks[:, 16:32].reshape(256, LATENT),
        gain_grad,
    )


def solution(mesh):
    split = Mesh(mesh.devices.reshape(4, 4, 4, 2), ("sp_0", "sp_1", "dp_0", "dp_1"))
    in_specs = (
        P(DP, SP, None),
        P(DP, SP, None),
        P(DP, SP, None),
        P(),
        P(DP, None),
        P(DP, None),
        P(DP, SP, None),
    )
    out_specs = (P(DP, SP, None), P(DP, SP, None), P(DP, SP, None), P(DP, None), P(DP, None), P())
    return jax.shard_map(local, mesh=split, in_specs=in_specs, out_specs=out_specs, check_vma=False)
```

```python
import functools

import jax
import jax.numpy as jnp
import numpy as np
from jax import lax
from jax.experimental import pallas as pl
from jax.experimental.pallas import tpu as pltpu
from jax.sharding import Mesh
from jax.sharding import PartitionSpec as P


PLAIN_HEAD_WIDTH = 64
ROPE = 32
SPAN = 64
LATENT = 1024
LENGTH = 3072
TOKENS = 192
DP = ("dp_0", "dp_1")
SP = ("sp_0", "sp_1")
SP_DP = ("sp_0", "sp_1", "dp_0", "dp_1")
SP_SIZE = 16
DP_SIZE = 8
BLOCK = 512
SCALE = (PLAIN_HEAD_WIDTH + ROPE) ** (-0.5)
LOG2E = 1.4426950408889634

eps = 1e-06
rope_base = 10000.0
f32 = jnp.float32
bf16 = jnp.bfloat16


def pack_tables():
    first = np.zeros((384 + 256 + 128, 512), np.float32)
    second = np.zeros((384 + 256 + 128, 256), np.float32)
    for t in range(2):
        q, d, r = 192 * t, 384 + 128 * t, 640
        for c in range(64):
            first[q + c, 256 * t + c] = 1
            first[d + c, 256 * t + 64 + c] = 1
            second[q + 96 + c, 128 * t + c] = 1
            second[d + 64 + c, 128 * t + 64 + c] = 1
        for c in range(32):
            first[q + 64 + c, 256 * t + 128 + c] = 1
            first[q + 160 + c, 256 * t + 160 + c] = 1
            first[r + c, 256 * t + 192 + c] = 1
    return first, second


def unpack_table():
    place = np.zeros((512, 384), np.float32)
    for t in range(2):
        for h in range(2):
            for c in range(96):
                place[256 * t + 128 * h + c, 192 * t + 96 * h + c] = 1
    return place


def rope_tables():
    swap = np.zeros((128, 128), np.float32)
    for g in range(3):
        for c in range(16):
            swap[32 * g + 16 + c, 32 * g + c] = -1
            swap[32 * g + c, 32 * g + 16 + c] = 1
    spread = np.zeros((128, 384), np.float32)
    for c in range(32):
        spread[c, c] = 1
        spread[32 + c, 128 + c] = 1
        spread[64 + c, 256 + c] = 1
    for c in range(16):
        spread[64 + 16 + c, 256 + 32 + c] = 1
        spread[64 + c, 256 + 32 + 16 + c] = -1
    return swap, spread


def pack_kernel(query, d_out, rope, first, second, out0, out1):
    both = jnp.concatenate([query[...], d_out[...], rope[...]], axis=1)
    one = jnp.dot(both, first[...], preferred_element_type=f32).astype(bf16)
    two = jnp.dot(both, second[...], preferred_element_type=f32).astype(bf16)
    for t in range(2):
        out0[t] = one[:, 256 * t : 256 * t + 256]
        out1[t] = two[:, 128 * t : 128 * t + 128]


def pack(query, d_out, rope):
    first, second = pack_tables()
    whole = lambda shape: pl.BlockSpec(shape, lambda j: (0, 0))
    return pl.pallas_call(
        pack_kernel,
        grid=(8,),
        in_specs=[
            pl.BlockSpec((TOKENS, 384), lambda j: (0, j)),
            pl.BlockSpec((TOKENS, 256), lambda j: (0, j)),
            whole((TOKENS, 128)),
            whole((768, 512)),
            whole((768, 256)),
        ],
        out_specs=[
            pl.BlockSpec((2, TOKENS, 256), lambda j: (j, 0, 0)),
            pl.BlockSpec((2, TOKENS, 128), lambda j: (j, 0, 0)),
        ],
        out_shape=[
            jax.ShapeDtypeStruct((SP_SIZE, TOKENS, 256), bf16),
            jax.ShapeDtypeStruct((SP_SIZE, TOKENS, 128), bf16),
        ],
        cost_estimate=pl.CostEstimate(
            flops=16 * 192 * 768 * 768, bytes_accessed=5_000_000, transcendentals=0
        ),
        name="pack",
    )(query, d_out, rope, jnp.asarray(first, bf16), jnp.asarray(second, bf16))


def dot_t(a, b):
    return lax.dot_general(a, b, (((1,), (1,)), ((), ())), preferred_element_type=f32)


def lanes(x, combine):
    parts = [x[:, k : k + 128] for k in range(0, x.shape[1], 128)]
    return functools.reduce(combine, parts)


def attention_kernel(a_ref, q2_ref, kv_ref, k2_ref, tab_ref, out_ref, s_ref, dp_ref, m_ref, l_ref, d_ref, dq_ref, acc_ref):
    step = pl.program_id(0)
    count = LENGTH // BLOCK
    i = count - 1 - step

    @pl.when(step == 0)
    def _():
        acc_ref[...] = jnp.zeros_like(acc_ref)

    rows = pl.ds(pl.multiple_of(i * BLOCK, BLOCK), BLOCK)
    a = a_ref[rows, :]
    q2 = q2_ref[rows, :]
    lane = lax.broadcasted_iota(jnp.int32, (BLOCK, 128), 1)
    nope = jnp.where(lane < 64, a, jnp.zeros_like(a))
    cot = jnp.where(lane < 64, jnp.zeros_like(a), a)
    query = jnp.concatenate([nope, q2], axis=1)
    a_t = a.T
    q2_t = q2.T
    left_k = jnp.concatenate([q2_t[0:32], a_t[0:64]], axis=0)
    left_v = a_t[64:128]

    def tile(j):
        return pl.ds(pl.multiple_of(j * BLOCK, BLOCK), BLOCK)

    def key(j):
        return jnp.concatenate([kv_ref[tile(j), :], k2_ref[tile(j), :]], axis=1)

    m_ref[...] = jnp.full_like(m_ref, -1e30)
    l_ref[...] = jnp.zeros_like(l_ref)
    d_ref[...] = jnp.zeros_like(d_ref)
    dq_ref[...] = jnp.zeros_like(dq_ref)

    def scores(j, masked):
        s = dot_t(query, key(j))
        if masked:
            r = lax.broadcasted_iota(jnp.int32, (BLOCK, BLOCK), 0) // SPAN
            c = lax.broadcasted_iota(jnp.int32, (BLOCK, BLOCK), 1) // SPAN
            s = jnp.where(c <= r, s, -1e30)
        s_ref[:, tile(j)] = s
        m_ref[...] = jnp.maximum(m_ref[...], lanes(s, jnp.maximum))

    @pl.loop(0, i)
    def _(j):
        scores(j, False)

    scores(i, True)
    m = jnp.max(m_ref[...], axis=1, keepdims=True)

    def weights(j):
        dp = dot_t(cot, kv_ref[tile(j), :])
        e = jnp.exp2((s_ref[:, tile(j)] - m) * (SCALE * LOG2E))
        l_ref[...] += lanes(e, jnp.add)
        d_ref[...] += lanes(e * dp, jnp.add)
        s_ref[:, tile(j)] = e
        dp_ref[:, tile(j)] = dp

    @pl.loop(0, i + 1)
    def _(j):
        weights(j)

    inverse = 1.0 / jnp.sum(l_ref[...], axis=1, keepdims=True)
    delta = jnp.sum(d_ref[...], axis=1, keepdims=True) * inverse

    @pl.loop(0, i + 1)
    def _(j):
        p = s_ref[:, tile(j)] * inverse
        ds = (p * (dp_ref[:, tile(j)] - delta)).astype(bf16)
        dq_ref[...] += jnp.dot(ds, key(j), preferred_element_type=f32)
        acc_ref[0:96, tile(j)] += jnp.dot(left_k, ds, preferred_element_type=f32)
        acc_ref[96:160, tile(j)] += jnp.dot(left_v, p.astype(bf16), preferred_element_type=f32)

    turned = dq_ref[:, 128:256] * tab_ref[...]
    turned = turned + pltpu.roll(turned, 96, 1)
    dq = jnp.where(lane < 64, dq_ref[:, 0:128], pltpu.roll(turned, 64, 1)) * SCALE
    done = acc_ref[:, rows]
    k_rope = done[0:32] * SCALE
    k_nope = done[32:96] * SCALE
    low = jnp.concatenate([jnp.zeros((96, BLOCK), f32), k_rope], axis=0).T
    out_ref[:, 0:128] = jnp.where(lane < 96, dq, low).astype(bf16)
    out_ref[:, 128:256] = jnp.concatenate([k_nope, done[96:160]], axis=0).T.astype(bf16)


def attention(a, q2, kv, k2, table):
    count = LENGTH // BLOCK
    whole = pl.BlockSpec((LENGTH, 128), lambda i: (0, 0))
    return pl.pallas_call(
        attention_kernel,
        grid=(count,),
        in_specs=[whole] * 4 + [pl.BlockSpec((BLOCK, 128), lambda i: (count - 1 - i, 0))],
        out_specs=pl.BlockSpec((BLOCK, 256), lambda i: (count - 1 - i, 0)),
        out_shape=jax.ShapeDtypeStruct((LENGTH, 256), bf16),
        scratch_shapes=[
            pltpu.VMEM((BLOCK, LENGTH), f32),
            pltpu.VMEM((BLOCK, LENGTH), f32),
            pltpu.VMEM((BLOCK, 128), f32),
            pltpu.VMEM((BLOCK, 128), f32),
            pltpu.VMEM((BLOCK, 128), f32),
            pltpu.VMEM((BLOCK, 256), f32),
            pltpu.VMEM((160, LENGTH), f32),
        ],
        compiler_params=pltpu.CompilerParams(
            dimension_semantics=("arbitrary",), vmem_limit_bytes=48 * 1024 * 1024
        ),
        cost_estimate=pl.CostEstimate(
            flops=12_000_000_000, bytes_accessed=8_000_000, transcendentals=5_000_000
        ),
        name="attention",
    )(a, q2, kv, k2, table)


def finish_kernel(ret0, ret1, w, place, latent, gain, query_grad, latent_grad, rope_sum, acc):
    step = pl.program_id(0)

    @pl.when(step == 0)
    def _():
        acc[...] = jnp.zeros_like(acc)
        rope_sum[...] = jnp.zeros_like(rope_sum)

    left = [ret[t, :, 0:128] for t in range(2) for ret in (ret0, ret1)]
    query_grad[...] = jnp.dot(
        jnp.concatenate(left, axis=1), place[...], preferred_element_type=f32
    ).astype(bf16)
    rope_sum[...] += sum(x.astype(f32) for x in left)
    total = acc[...]
    for t in range(2):
        right = jnp.concatenate([ret0[t, :, 128:256], ret1[t, :, 128:256]], axis=1)
        total += jnp.dot(right, w[t], preferred_element_type=f32)
    acc[...] = total

    @pl.when(step == pl.num_programs(0) - 1)
    def _():
        lat = latent[...].astype(f32)
        inverse = lax.rsqrt(jnp.mean(lat * lat, axis=1, keepdims=True) + eps)
        normed = lat * inverse
        scaled = acc[...] * gain[...]
        latent_grad[...] = inverse * (
            scaled - normed * jnp.mean(scaled * normed, axis=1, keepdims=True)
        )


def finish(ret0, ret1, w, latent, gain):
    fixed = lambda shape: pl.BlockSpec(shape, lambda j: (0,) * len(shape))
    return pl.pallas_call(
        finish_kernel,
        grid=(8,),
        in_specs=[
            pl.BlockSpec((2, TOKENS, 256), lambda j: (j, 0, 0)),
            pl.BlockSpec((2, TOKENS, 256), lambda j: (j, 0, 0)),
            pl.BlockSpec((2, 256, LATENT), lambda j: (j, 0, 0)),
            fixed((512, 384)),
            fixed((TOKENS, LATENT)),
            fixed((1, LATENT)),
        ],
        out_specs=[
            pl.BlockSpec((TOKENS, 384), lambda j: (0, j)),
            fixed((TOKENS, LATENT)),
            fixed((TOKENS, 128)),
        ],
        out_shape=[
            jax.ShapeDtypeStruct((TOKENS, 3072), bf16),
            jax.ShapeDtypeStruct((TOKENS, LATENT), f32),
            jax.ShapeDtypeStruct((TOKENS, 128), f32),
        ],
        scratch_shapes=[pltpu.VMEM((TOKENS, LATENT), f32)],
        compiler_params=pltpu.CompilerParams(dimension_semantics=("arbitrary",)),
        cost_estimate=pl.CostEstimate(
            flops=4_000_000_000, bytes_accessed=14_000_000, transcendentals=0
        ),
        name="finish",
    )(ret0, ret1, w, jnp.asarray(unpack_table(), bf16), latent, gain)


def rotate(values, cosine, sine):
    half = values.shape[-1] // 2
    first = values[..., :half]
    second = values[..., half:]
    return jnp.concatenate(
        [first * cosine - second * sine, second * cosine + first * sine], axis=-1
    )


def inverse_frequency(index):
    return 1.0 / rope_base ** (2.0 * index.astype(f32) / ROPE)


def to_heads():
    pairs = []
    for i in range(DP_SIZE):
        for n in range(DP_SIZE):
            for b in range(2):
                pairs.append(((8 * b + n) * DP_SIZE + i, (2 * i + b) * DP_SIZE + n))
    return pairs


def spread_kernel(with_messages, *refs):
    if with_messages:
        x, msgs, full, got, own_sem, leg_send, leg_recv, far_send, far_recv, msg_send, msg_recv = refs
    else:
        x, full, own_sem, leg_send, leg_recv, far_send, far_recv = refs
    z, y = lax.axis_index("sp_0"), lax.axis_index("sp_1")
    me = 4 * z + y
    size = x.shape[0] // 2

    def at(dz, dy):
        return {"sp_0": lax.rem(z + dz, 4), "sp_1": lax.rem(y + dy, 4)}

    barrier = pltpu.get_barrier_semaphore()
    for k in range(1, SP_SIZE):
        pl.semaphore_signal(
            barrier, inc=1, device_id=at(k // 4, k % 4), device_id_type=pl.DeviceIdType.MESH
        )
    pl.semaphore_wait(barrier, SP_SIZE - 1)

    def copy(src, dst, send, recv, where):
        c = pltpu.make_async_remote_copy(
            src_ref=src,
            dst_ref=dst,
            send_sem=send,
            recv_sem=recv,
            device_id=where,
            device_id_type=pl.DeviceIdType.MESH,
        )
        c.start()
        return c

    steps = (1, 3, 2)
    halves = (pl.ds(0, size), pl.ds(size, size))
    own = [pltpu.make_async_copy(x, full.at[me], own_sem.at[0])]
    if with_messages:
        own.append(pltpu.make_async_copy(msgs.at[me], got.at[me], own_sem.at[1]))
    near = {}
    far = []
    for d in steps:
        for h in range(2):
            where = at(0, d) if h == 0 else at(d, 0)
            near[h, d] = copy(
                x.at[halves[h]],
                full.at[me, halves[h]],
                leg_send.at[h, d - 1],
                leg_recv.at[h, d - 1],
                where,
            )
    for c in own:
        c.start()
    for e in steps:
        for h in range(2):
            where = at(e, 0) if h == 0 else at(0, e)
            far.append(
                copy(
                    x.at[halves[h]],
                    full.at[me, halves[h]],
                    far_send.at[h, 0, e - 1],
                    far_recv.at[h, 0, e - 1],
                    where,
                )
            )
    if with_messages:
        for k in range(1, SP_SIZE):
            there = 4 * lax.rem(z + k // 4, 4) + lax.rem(y + k % 4, 4)
            far.append(
                copy(
                    msgs.at[there],
                    got.at[me],
                    msg_send.at[k - 1],
                    msg_recv.at[k - 1],
                    at(k // 4, k % 4),
                )
            )
    for d in steps:
        for h in range(2):
            near[h, d].wait_recv()
            if h == 0:
                source = 4 * z + lax.rem(y + 4 - d, 4)
            else:
                source = 4 * lax.rem(z + 4 - d, 4) + y
            block = full.at[source, halves[h]]
            for e in steps:
                where = at(e, 0) if h == 0 else at(0, e)
                far.append(
                    copy(block, block, far_send.at[h, d, e - 1], far_recv.at[h, d, e - 1], where)
                )
    for c in near.values():
        c.wait_send()
    for c in far:
        c.wait()
    for c in own:
        c.wait()


def spread_over_sp(x, msgs, collective_id):
    with_messages = msgs is not None
    vmem = pl.BlockSpec(memory_space=pltpu.VMEM)
    anywhere = pl.BlockSpec(memory_space=pl.ANY)
    out_shape = [jax.ShapeDtypeStruct((SP_SIZE, *x.shape), x.dtype)]
    dma = pltpu.SemaphoreType.DMA
    scratch = [dma((2,)), dma((2, 3)), dma((2, 3)), dma((2, 4, 3)), dma((2, 4, 3))]
    if with_messages:
        out_shape.append(jax.ShapeDtypeStruct(msgs.shape, msgs.dtype))
        scratch += [dma((SP_SIZE - 1,)), dma((SP_SIZE - 1,))]
    return pl.pallas_call(
        functools.partial(spread_kernel, with_messages),
        in_specs=[vmem] * (1 + with_messages),
        out_specs=[anywhere] * (1 + with_messages),
        out_shape=out_shape,
        scratch_shapes=scratch,
        compiler_params=pltpu.CompilerParams(collective_id=collective_id, has_side_effects=True),
        cost_estimate=pl.CostEstimate(
            flops=8_000_000_000, bytes_accessed=8_000_000, transcendentals=0
        ),
        name="spread",
    )(*((x, msgs) if with_messages else (x,)))


def exchange(value):
    return lax.all_to_all(value, SP, split_axis=0, concat_axis=0, tiled=True)


def layer(query, latent, rope_key, latent_norm_gain, key_up_matrix, value_up_matrix, out_grad):
    lat = latent[0].astype(f32)
    inv_rms = lax.rsqrt(jnp.mean(lat * lat, axis=-1, keepdims=True) + eps)
    nlat = (lat * inv_rms * latent_norm_gain).astype(bf16)

    shard = jnp.stack(
        [key_up_matrix.reshape(2, 2, 64, LATENT), value_up_matrix.reshape(2, 2, 64, LATENT)],
        axis=2,
    ).reshape(2, 256, LATENT)
    spot = lax.axis_index(SP)
    half = lax.dynamic_index_in_dim(shard, spot // 8, 0, keepdims=False)
    w_own = lax.ppermute(half, SP_DP, to_heads())
    w_whole = lax.all_gather(shard, DP, axis=0, tiled=True)

    rope_wide = jnp.pad(rope_key[0], ((0, 0), (0, 96)))
    sent0, sent1 = pack(query[0], out_grad[0], rope_wide)
    nlat_full, got0 = spread_over_sp(nlat, sent0, 0)
    nlat_full = nlat_full.reshape(LENGTH, LATENT)
    got0 = got0.reshape(LENGTH, 256)
    sent1, got0 = lax.optimization_barrier((sent1, got0))
    got1 = exchange(sent1).reshape(LENGTH, 128)

    column = jnp.arange(128)
    turned = jnp.arange(LENGTH, dtype=f32)[:, None] * inverse_frequency(column % 16)[None, :]
    cosine = jnp.cos(turned)
    sine = jnp.sin(turned)
    table = jnp.where(column < 32, cosine, jnp.where(column < 64, sine, 0.0))
    swap, spread = rope_tables()

    raw = got0[:, 128:256]
    swapped = jnp.dot(raw, jnp.asarray(swap, bf16), preferred_element_type=f32)
    rotated = (raw.astype(f32) * cosine + swapped * sine).astype(bf16)
    apart = jnp.dot(rotated, jnp.asarray(spread, bf16), preferred_element_type=f32).astype(bf16)
    q2_0, q2_1, k2 = apart[:, 0:128], apart[:, 128:256], apart[:, 256:384]

    kv = lax.dot_general(
        nlat_full, w_own, (((1,), (1,)), ((), ())), preferred_element_type=f32
    ).astype(bf16)

    def weight_part(grads, h):
        d_w = lax.dot_general(
            grads[:, 128:256], nlat_full, (((0,), (0,)), ((), ())), preferred_element_type=f32
        )
        own = w_own[128 * h : 128 * h + 128].astype(f32)
        gain_part = jnp.sum(d_w * own, axis=0)
        pieces = (
            d_w.reshape(2, DP_SIZE, 8, LATENT)
            .transpose(1, 0, 2, 3)
            .reshape(DP_SIZE, 16, LATENT)
        )
        arrived = lax.psum_scatter(pieces, DP, scatter_dimension=0, tiled=True)[0]
        return arrived, gain_part

    grads0 = attention(got0[:, 0:128], q2_0, kv[:, 0:128], k2, table)
    grads0, got1 = lax.optimization_barrier((grads0, got1))
    ret0 = exchange(grads0.reshape(SP_SIZE, TOKENS, 256))
    arrived0, gain0 = weight_part(grads0, 0)
    grads1 = attention(got1, q2_1, kv[:, 128:256], k2, table)
    grads1, ret0 = lax.optimization_barrier((grads1, ret0))
    ret1 = exchange(grads1.reshape(SP_SIZE, TOKENS, 256))
    arrived1, gain1 = weight_part(grads1, 1)
    piece = jnp.concatenate([arrived0, arrived1], axis=0)
    moved = lax.ppermute(piece, SP_DP, [(b, a) for a, b in to_heads()])
    gain_grad = lax.psum((gain0 + gain1) / latent_norm_gain, SP_DP)
    (blocks,) = spread_over_sp(moved, None, 1)

    query_grad, latent_grad, rope_sum = finish(
        ret0, ret1, w_whole, latent[0], latent_norm_gain[None]
    )
    position = (spot * TOKENS + jnp.arange(TOKENS)).astype(f32)
    angle = position[:, None] * inverse_frequency(jnp.arange(16))[None, :]
    rope_grad = rotate(rope_sum[:, 96:128], jnp.cos(angle), -jnp.sin(angle))
    blocks = blocks.reshape(2, DP_SIZE, 2, 2, 8, LATENT).transpose(3, 0, 2, 1, 4, 5)
    blocks = blocks.reshape(2, 256, LATENT)
    return (
        query_grad[None],
        latent_grad[None],
        rope_grad[None],
        blocks[0],
        blocks[1],
        gain_grad,
    )


def solution(mesh):
    split = Mesh(mesh.devices.reshape(4, 4, 4, 2), ("sp_0", "sp_1", "dp_0", "dp_1"))
    in_specs = (
        P(DP, SP, None),
        P(DP, SP, None),
        P(DP, SP, None),
        P(),
        P(DP, None),
        P(DP, None),
        P(DP, SP, None),
    )
    out_specs = (P(DP, SP, None), P(DP, SP, None), P(DP, SP, None), P(DP, None), P(DP, None), P())
    return jax.shard_map(layer, mesh=split, in_specs=in_specs, out_specs=out_specs, check_vma=False)
```

```python
import functools

import jax
import jax.numpy as jnp
import numpy as np
from jax import lax
from jax.experimental import pallas as pl
from jax.experimental.pallas import tpu as pltpu
from jax.sharding import Mesh
from jax.sharding import PartitionSpec as P


PLAIN_HEAD_WIDTH = 64
ROPE = 32
SPAN = 64
LATENT = 1024
LENGTH = 3072
TOKENS = 192
DP = ("dp_0", "dp_1")
SP = ("sp_0", "sp_1")
SP_DP = ("sp_0", "sp_1", "dp_0", "dp_1")
SP_SIZE = 16
DP_SIZE = 8
BLOCK = 512
SCALE = (PLAIN_HEAD_WIDTH + ROPE) ** (-0.5)
LOG2E = 1.4426950408889634

eps = 1e-06
rope_base = 10000.0
f32 = jnp.float32
bf16 = jnp.bfloat16


def pack_tables():
    first = np.zeros((384 + 256 + 128, 512), np.float32)
    second = np.zeros((384 + 256 + 128, 256), np.float32)
    for t in range(2):
        q, d, r = 192 * t, 384 + 128 * t, 640
        for c in range(64):
            first[q + c, 256 * t + c] = 1
            first[d + c, 256 * t + 64 + c] = 1
            second[q + 96 + c, 128 * t + c] = 1
            second[d + 64 + c, 128 * t + 64 + c] = 1
        for c in range(32):
            first[q + 64 + c, 256 * t + 128 + c] = 1
            first[q + 160 + c, 256 * t + 160 + c] = 1
            first[r + c, 256 * t + 192 + c] = 1
    return first, second


def unpack_tables():
    place = np.zeros((512, 384), np.float32)
    turn = np.zeros((512, 384), np.float32)
    for t in range(2):
        for h in range(2):
            row, col = 256 * t + 128 * h, 192 * t + 96 * h
            for c in range(96):
                place[row + c, col + c] = 1
            for c in range(64, 80):
                turn[row + c + 16, col + c] = 1
                turn[row + c, col + c + 16] = -1
    return place, turn


def rope_table():
    spread = np.zeros((128, 384), np.float32)
    for c in range(32):
        spread[c, c] = 1
        spread[32 + c, 128 + c] = 1
        spread[64 + c, 256 + c] = 1
    return spread


def turned_halves(x):
    lane = lax.broadcasted_iota(jnp.int32, x.shape, 1)
    return jnp.where(lane % 32 < 16, -pltpu.roll(x, 112, 1), pltpu.roll(x, 16, 1))


def pack_kernel(query, d_out, rope, first, second, cosine, sine, out0, out1):
    both = jnp.concatenate([query[...], d_out[...], rope[...]], axis=1)
    one = jnp.dot(both, first[...], preferred_element_type=f32)
    two = jnp.dot(both, second[...], preferred_element_type=f32).astype(bf16)
    for t in range(2):
        out0[t, :, 0:128] = one[:, 256 * t : 256 * t + 128].astype(bf16)
        raw = one[:, 256 * t + 128 : 256 * t + 256]
        out0[t, :, 128:256] = (raw * cosine[...] + turned_halves(raw) * sine[...]).astype(bf16)
        out1[t] = two[:, 128 * t : 128 * t + 128]


def pack(query, d_out, rope, cosine, sine):
    first, second = pack_tables()
    whole = lambda shape: pl.BlockSpec(shape, lambda j: (0, 0))
    return pl.pallas_call(
        pack_kernel,
        grid=(8,),
        in_specs=[
            pl.BlockSpec((TOKENS, 384), lambda j: (0, j)),
            pl.BlockSpec((TOKENS, 256), lambda j: (0, j)),
            whole((TOKENS, 128)),
            whole((768, 512)),
            whole((768, 256)),
            whole((TOKENS, 128)),
            whole((TOKENS, 128)),
        ],
        out_specs=[
            pl.BlockSpec((2, TOKENS, 256), lambda j: (j, 0, 0)),
            pl.BlockSpec((2, TOKENS, 128), lambda j: (j, 0, 0)),
        ],
        out_shape=[
            jax.ShapeDtypeStruct((SP_SIZE, TOKENS, 256), bf16),
            jax.ShapeDtypeStruct((SP_SIZE, TOKENS, 128), bf16),
        ],
        cost_estimate=pl.CostEstimate(
            flops=16 * 192 * 768 * 768, bytes_accessed=5_000_000, transcendentals=0
        ),
        name="pack",
    )(query, d_out, rope, jnp.asarray(first, bf16), jnp.asarray(second, bf16), cosine, sine)


def dot_t(a, b):
    return lax.dot_general(a, b, (((1,), (1,)), ((), ())), preferred_element_type=f32)


def lanes(x, combine):
    parts = [x[:, k : k + 128] for k in range(0, x.shape[1], 128)]
    return functools.reduce(combine, parts)


def attention_kernel(a_ref, q2_ref, kv_ref, k2_ref, out_ref, s_ref, dp_ref, m_ref, l_ref, d_ref, dq_ref, acc_ref):
    step = pl.program_id(0)
    count = LENGTH // BLOCK
    i = count - 1 - step

    @pl.when(step == 0)
    def _():
        acc_ref[...] = jnp.zeros_like(acc_ref)

    rows = pl.ds(pl.multiple_of(i * BLOCK, BLOCK), BLOCK)
    a = a_ref[rows, :]
    q2 = q2_ref[rows, :]
    lane = lax.broadcasted_iota(jnp.int32, (BLOCK, 128), 1)
    nope = jnp.where(lane < 64, a, jnp.zeros_like(a))
    cot = jnp.where(lane < 64, jnp.zeros_like(a), a)
    query = jnp.concatenate([nope, q2], axis=1)
    a_t = a.T
    q2_t = q2.T
    left_k = jnp.concatenate([q2_t[0:32], a_t[0:64]], axis=0)
    left_v = a_t[64:128]

    def tile(j):
        return pl.ds(pl.multiple_of(j * BLOCK, BLOCK), BLOCK)

    def key(j):
        return jnp.concatenate([kv_ref[tile(j), :], k2_ref[tile(j), :]], axis=1)

    m_ref[...] = jnp.full_like(m_ref, -1e30)
    l_ref[...] = jnp.zeros_like(l_ref)
    d_ref[...] = jnp.zeros_like(d_ref)
    dq_ref[...] = jnp.zeros_like(dq_ref)

    def scores(j, masked):
        s = dot_t(query, key(j))
        if masked:
            r = lax.broadcasted_iota(jnp.int32, (BLOCK, BLOCK), 0) // SPAN
            c = lax.broadcasted_iota(jnp.int32, (BLOCK, BLOCK), 1) // SPAN
            s = jnp.where(c <= r, s, -1e30)
        s_ref[:, tile(j)] = s
        m_ref[...] = jnp.maximum(m_ref[...], lanes(s, jnp.maximum))

    @pl.loop(0, i)
    def _(j):
        scores(j, False)

    scores(i, True)
    m = jnp.max(m_ref[...], axis=1, keepdims=True)

    def weights(j):
        dp = dot_t(cot, kv_ref[tile(j), :])
        e = jnp.exp2((s_ref[:, tile(j)] - m) * (SCALE * LOG2E))
        l_ref[...] += lanes(e, jnp.add)
        d_ref[...] += lanes(e * dp, jnp.add)
        s_ref[:, tile(j)] = e
        dp_ref[:, tile(j)] = dp

    @pl.loop(0, i + 1)
    def _(j):
        weights(j)

    inverse = 1.0 / jnp.sum(l_ref[...], axis=1, keepdims=True)
    delta = jnp.sum(d_ref[...], axis=1, keepdims=True) * inverse

    @pl.loop(0, i + 1)
    def _(j):
        p = s_ref[:, tile(j)] * inverse
        ds = (p * (dp_ref[:, tile(j)] - delta)).astype(bf16)
        dq_ref[...] += jnp.dot(ds, key(j), preferred_element_type=f32)
        acc_ref[0:96, tile(j)] += jnp.dot(left_k, ds, preferred_element_type=f32)
        acc_ref[96:160, tile(j)] += jnp.dot(left_v, p.astype(bf16), preferred_element_type=f32)

    dq = jnp.where(lane < 64, dq_ref[:, 0:128], pltpu.roll(dq_ref[:, 128:256], 64, 1)) * SCALE
    done = acc_ref[:, rows]
    k_rope = done[0:32] * SCALE
    k_nope = done[32:96] * SCALE
    low = jnp.concatenate([jnp.zeros((96, BLOCK), f32), k_rope], axis=0).T
    out_ref[:, 0:128] = jnp.where(lane < 96, dq, low).astype(bf16)
    out_ref[:, 128:256] = jnp.concatenate([k_nope, done[96:160]], axis=0).T.astype(bf16)


def attention(a, kv, ropes, head):
    count = LENGTH // BLOCK

    def column(k):
        return pl.BlockSpec((LENGTH, 128), lambda i: (0, k))

    return pl.pallas_call(
        attention_kernel,
        grid=(count,),
        in_specs=[column(0), column(head), column(head), column(2)],
        out_specs=pl.BlockSpec((BLOCK, 256), lambda i: (count - 1 - i, 0)),
        out_shape=jax.ShapeDtypeStruct((LENGTH, 256), bf16),
        scratch_shapes=[
            pltpu.VMEM((BLOCK, LENGTH), f32),
            pltpu.VMEM((BLOCK, LENGTH), f32),
            pltpu.VMEM((BLOCK, 128), f32),
            pltpu.VMEM((BLOCK, 128), f32),
            pltpu.VMEM((BLOCK, 128), f32),
            pltpu.VMEM((BLOCK, 256), f32),
            pltpu.VMEM((160, LENGTH), f32),
        ],
        compiler_params=pltpu.CompilerParams(
            dimension_semantics=("arbitrary",), vmem_limit_bytes=48 * 1024 * 1024
        ),
        cost_estimate=pl.CostEstimate(
            flops=12_000_000_000, bytes_accessed=8_000_000, transcendentals=5_000_000
        ),
        name="attention",
    )(a, ropes, kv, ropes)


def finish_kernel(
    ret0, ret1, w, place, turn, latent, gain, wide_cos, wide_sin, cosine, sine,
    query_grad, latent_grad, rope_sum, acc,
):
    step = pl.program_id(0)

    @pl.when(step == 0)
    def _():
        acc[...] = jnp.zeros_like(acc)
        rope_sum[...] = jnp.zeros_like(rope_sum)

    left = [ret[t, :, 0:128] for t in range(2) for ret in (ret0, ret1)]
    row = jnp.concatenate(left, axis=1)
    plain = jnp.dot(row, place[...], preferred_element_type=f32)
    turned = jnp.dot(row, turn[...], preferred_element_type=f32)
    query_grad[...] = (plain * wide_cos[...] + turned * wide_sin[...]).astype(bf16)
    rope_sum[...] += sum(x.astype(f32) for x in left)
    total = acc[...]
    for t in range(2):
        right = jnp.concatenate([ret0[t, :, 128:256], ret1[t, :, 128:256]], axis=1)
        total += jnp.dot(right, w[t], preferred_element_type=f32)
    acc[...] = total

    @pl.when(step == pl.num_programs(0) - 1)
    def _():
        lat = latent[...].astype(f32)
        inverse = lax.rsqrt(jnp.mean(lat * lat, axis=1, keepdims=True) + eps)
        normed = lat * inverse
        scaled = acc[...] * gain[...]
        latent_grad[...] = inverse * (
            scaled - normed * jnp.mean(scaled * normed, axis=1, keepdims=True)
        )
        total_rope = rope_sum[...]
        rope_sum[...] = total_rope * cosine[...] - turned_halves(total_rope) * sine[...]


def finish(ret0, ret1, w, latent, gain, wide_cos, wide_sin, cosine, sine):
    fixed = lambda shape: pl.BlockSpec(shape, lambda j: (0,) * len(shape))
    place, turn = unpack_tables()
    return pl.pallas_call(
        finish_kernel,
        grid=(8,),
        in_specs=[
            pl.BlockSpec((2, TOKENS, 256), lambda j: (j, 0, 0)),
            pl.BlockSpec((2, TOKENS, 256), lambda j: (j, 0, 0)),
            pl.BlockSpec((2, 256, LATENT), lambda j: (j, 0, 0)),
            fixed((512, 384)),
            fixed((512, 384)),
            fixed((TOKENS, LATENT)),
            fixed((1, LATENT)),
            fixed((TOKENS, 384)),
            fixed((TOKENS, 384)),
            fixed((TOKENS, 128)),
            fixed((TOKENS, 128)),
        ],
        out_specs=[
            pl.BlockSpec((TOKENS, 384), lambda j: (0, j)),
            fixed((TOKENS, LATENT)),
            fixed((TOKENS, 128)),
        ],
        out_shape=[
            jax.ShapeDtypeStruct((TOKENS, 3072), bf16),
            jax.ShapeDtypeStruct((TOKENS, LATENT), f32),
            jax.ShapeDtypeStruct((TOKENS, 128), f32),
        ],
        scratch_shapes=[pltpu.VMEM((TOKENS, LATENT), f32)],
        compiler_params=pltpu.CompilerParams(dimension_semantics=("arbitrary",)),
        cost_estimate=pl.CostEstimate(
            flops=4_000_000_000, bytes_accessed=14_000_000, transcendentals=0
        ),
        name="finish",
    )(
        ret0, ret1, w, jnp.asarray(place, bf16), jnp.asarray(turn, bf16), latent, gain,
        wide_cos, wide_sin, cosine, sine,
    )


def inverse_frequency(index):
    return 1.0 / rope_base ** (2.0 * index.astype(f32) / ROPE)


def to_heads():
    pairs = []
    for i in range(DP_SIZE):
        for n in range(DP_SIZE):
            for b in range(2):
                pairs.append(((8 * b + n) * DP_SIZE + i, (2 * i + b) * DP_SIZE + n))
    return pairs


def spread_kernel(with_messages, *refs):
    count = 2 if with_messages else 1
    x, full = refs[0], refs[count]
    own_sem, leg, leg_in, pass1, pass1_in, far, far_in, pass2, pass2_in = refs[2 * count : 2 * count + 9]
    if with_messages:
        msgs, got = refs[1], refs[3]
        msg_send, msg_recv = refs[2 * count + 9 :]
    z, y = lax.axis_index("sp_0"), lax.axis_index("sp_1")
    me = 4 * z + y
    size = x.shape[0] // 2

    def at(dz, dy):
        return {"sp_0": lax.rem(z + dz, 4), "sp_1": lax.rem(y + dy, 4)}

    def along(h, s):
        return at(0, s) if h == 0 else at(s, 0)

    def across(h, s):
        return at(s, 0) if h == 0 else at(0, s)

    def block(h, s, c):
        dz, dy = (c, s) if h == 0 else (s, c)
        return 4 * lax.rem(z + dz, 4) + lax.rem(y + dy, 4)

    if with_messages:
        peers = [(k // 4, k % 4) for k in range(1, SP_SIZE)]
    else:
        peers = [(0, 1), (0, 3), (1, 0), (3, 0)]
    barrier = pltpu.get_barrier_semaphore()
    for dz, dy in peers:
        pl.semaphore_signal(
            barrier, inc=1, device_id=at(dz, dy), device_id_type=pl.DeviceIdType.MESH
        )
    pl.semaphore_wait(barrier, len(peers))

    def copy(src, dst, send, recv, where):
        c = pltpu.make_async_remote_copy(
            src_ref=src,
            dst_ref=dst,
            send_sem=send,
            recv_sem=recv,
            device_id=where,
            device_id_type=pl.DeviceIdType.MESH,
        )
        c.start()
        return c

    half = [pl.ds(h * size, size) for h in range(2)]
    quarter = [[pl.ds(h * size + q * size // 2, size // 2) for q in range(2)] for h in range(2)]
    ways = (1, 3)
    lines = (0, 3, 1, 2)
    first, second, third, fourth, rest = {}, {}, {}, {}, []
    for w, s in enumerate(ways):
        for h in range(2):
            first[h, w] = copy(
                x.at[half[h]], full.at[me, half[h]], leg.at[h, w], leg_in.at[h, w], along(h, s)
            )
    for w, s in enumerate(ways):
        for h in range(2):
            third[h, 0, w] = copy(
                x.at[half[h]], full.at[me, half[h]], far.at[h, 0, w], far_in.at[h, 0, w], across(h, s)
            )
    own = [pltpu.make_async_copy(x, full.at[me], own_sem.at[0])]
    if with_messages:
        own.append(pltpu.make_async_copy(msgs.at[me], got.at[me], own_sem.at[1]))
    for c in own:
        c.start()
    if with_messages:
        for k, (dz, dy) in enumerate(peers):
            rest.append(
                copy(
                    msgs.at[block(0, dy, dz)],
                    got.at[me],
                    msg_send.at[k],
                    msg_recv.at[k],
                    at(dz, dy),
                )
            )

    def onward(h, k):
        there = full.at[block(h, lines[k], 0), half[h]]
        for w, s in enumerate(ways):
            third[h, k, w] = copy(there, there, far.at[h, k, w], far_in.at[h, k, w], across(h, s))

    for w, s in enumerate(ways):
        for h in range(2):
            first[h, w].wait_recv()
            piece = full.at[block(h, 4 - s, 0), quarter[h][w]]
            second[h, w] = copy(piece, piece, pass1.at[h, w], pass1_in.at[h, w], along(h, s))
            onward(h, w + 1)
    for h in range(2):
        for w in range(2):
            second[h, w].wait_recv()
        onward(h, 3)
    for k in range(4):
        for w, s in enumerate(ways):
            for h in range(2):
                third[h, k, w].wait_recv()
                piece = full.at[block(h, lines[k], 4 - s), quarter[h][w]]
                fourth[h, k, w] = copy(
                    piece, piece, pass2.at[h, k, w], pass2_in.at[h, k, w], across(h, s)
                )
    for group in (first, second, third):
        for c in group.values():
            c.wait_send()
    for c in fourth.values():
        c.wait()
    for c in rest + own:
        c.wait()


def spread_over_sp(x, msgs, collective_id):
    with_messages = msgs is not None
    vmem = pl.BlockSpec(memory_space=pltpu.VMEM)
    anywhere = pl.BlockSpec(memory_space=pl.ANY)
    out_shape = [jax.ShapeDtypeStruct((SP_SIZE, *x.shape), x.dtype)]
    dma = pltpu.SemaphoreType.DMA
    scratch = [dma((2,))] + [dma((2, 2))] * 4 + [dma((2, 4, 2))] * 4
    if with_messages:
        out_shape.append(jax.ShapeDtypeStruct(msgs.shape, msgs.dtype))
        scratch += [dma((SP_SIZE - 1,)), dma((SP_SIZE - 1,))]
    return pl.pallas_call(
        functools.partial(spread_kernel, with_messages),
        in_specs=[vmem] * (1 + with_messages),
        out_specs=[anywhere] * (1 + with_messages),
        out_shape=out_shape,
        scratch_shapes=scratch,
        compiler_params=pltpu.CompilerParams(collective_id=collective_id, has_side_effects=True),
        cost_estimate=pl.CostEstimate(
            flops=8_000_000_000, bytes_accessed=8_000_000, transcendentals=0
        ),
        name="spread",
    )(*((x, msgs) if with_messages else (x,)))


def exchange(value):
    return lax.all_to_all(value, SP, split_axis=0, concat_axis=0, tiled=True)


def layer(query, latent, rope_key, latent_norm_gain, key_up_matrix, value_up_matrix, out_grad):
    lat = latent[0].astype(f32)
    inv_rms = lax.rsqrt(jnp.mean(lat * lat, axis=-1, keepdims=True) + eps)
    nlat = (lat * inv_rms * latent_norm_gain).astype(bf16)

    shard = jnp.stack(
        [key_up_matrix.reshape(2, 2, 64, LATENT), value_up_matrix.reshape(2, 2, 64, LATENT)],
        axis=2,
    ).reshape(2, 256, LATENT)
    spot = lax.axis_index(SP)
    half = lax.dynamic_index_in_dim(shard, spot // 8, 0, keepdims=False)
    w_own = lax.ppermute(half, SP_DP, to_heads())
    w_whole = lax.all_gather(shard, DP, axis=0, tiled=True)

    position = (spot * TOKENS + jnp.arange(TOKENS)).astype(f32)[:, None]
    angle = position * inverse_frequency(jnp.arange(128) % 16)[None]
    cosine, sine = jnp.cos(angle), jnp.sin(angle)
    place = jnp.arange(384) % 96
    wide = position * jnp.where(place < 64, 0.0, inverse_frequency(place % 16))[None]
    wide_cos, wide_sin = jnp.cos(wide), jnp.sin(wide)

    rope_wide = jnp.pad(rope_key[0], ((0, 0), (0, 96)))
    sent0, sent1 = pack(query[0], out_grad[0], rope_wide, cosine, sine)
    nlat_full, got0 = spread_over_sp(nlat, sent0, 0)
    nlat_full = nlat_full.reshape(LENGTH, LATENT)
    got0 = got0.reshape(LENGTH, 256)
    sent1, got0 = lax.optimization_barrier((sent1, got0))
    got1 = exchange(sent1).reshape(LENGTH, 128)

    ropes = jnp.dot(
        got0[:, 128:256], jnp.asarray(rope_table(), bf16), preferred_element_type=f32
    ).astype(bf16)
    kv = lax.dot_general(
        nlat_full, w_own, (((1,), (1,)), ((), ())), preferred_element_type=f32
    ).astype(bf16)

    def weight_part(grads, h):
        d_w = lax.dot_general(
            grads[:, 128:256], nlat_full, (((0,), (0,)), ((), ())), preferred_element_type=f32
        )
        own = w_own[128 * h : 128 * h + 128].astype(f32)
        gain_part = jnp.sum(d_w * own, axis=0)
        pieces = (
            d_w.reshape(2, DP_SIZE, 8, LATENT)
            .transpose(1, 0, 2, 3)
            .reshape(DP_SIZE, 16, LATENT)
        )
        arrived = lax.psum_scatter(pieces, DP, scatter_dimension=0, tiled=True)[0]
        return arrived, gain_part

    grads0 = attention(got0, kv, ropes, 0)
    grads0, got1 = lax.optimization_barrier((grads0, got1))
    ret0 = exchange(grads0.reshape(SP_SIZE, TOKENS, 256))
    arrived0, gain0 = weight_part(grads0, 0)
    grads1 = attention(got1, kv, ropes, 1)
    grads1, ret0 = lax.optimization_barrier((grads1, ret0))
    ret1 = exchange(grads1.reshape(SP_SIZE, TOKENS, 256))
    arrived1, gain1 = weight_part(grads1, 1)
    piece = jnp.concatenate([arrived0, arrived1], axis=0)
    moved = lax.ppermute(piece, SP_DP, [(b, a) for a, b in to_heads()])
    gain_grad = functools.reduce(lax.psum, SP_DP, (gain0 + gain1) / latent_norm_gain)
    (blocks,) = spread_over_sp(moved, None, 1)

    query_grad, latent_grad, rope_sum = finish(
        ret0, ret1, w_whole, latent[0], latent_norm_gain[None], wide_cos, wide_sin, cosine, sine
    )
    blocks = blocks.reshape(2, DP_SIZE, 2, 2, 8, LATENT).transpose(3, 0, 2, 1, 4, 5)
    blocks = blocks.reshape(2, 256, LATENT)
    return (
        query_grad[None],
        latent_grad[None],
        rope_sum[None, :, 96:128],
        blocks[0],
        blocks[1],
        gain_grad,
    )


def solution(mesh):
    split = Mesh(mesh.devices.reshape(4, 4, 4, 2), ("sp_0", "sp_1", "dp_0", "dp_1"))
    in_specs = (
        P(DP, SP, None),
        P(DP, SP, None),
        P(DP, SP, None),
        P(),
        P(DP, None),
        P(DP, None),
        P(DP, SP, None),
    )
    out_specs = (P(DP, SP, None), P(DP, SP, None), P(DP, SP, None), P(DP, None), P(DP, None), P())
    return jax.shard_map(layer, mesh=split, in_specs=in_specs, out_specs=out_specs, check_vma=False)
```

```python
import functools

import jax
import jax.numpy as jnp
import numpy as np
from jax import lax
from jax.experimental import pallas as pl
from jax.experimental.pallas import tpu as pltpu
from jax.sharding import Mesh
from jax.sharding import PartitionSpec as P


PLAIN_HEAD_WIDTH = 64
ROPE = 32
SPAN = 64
LATENT = 1024
LENGTH = 3072
TOKENS = 192
DP = ("dp_0", "dp_1")
SP = ("sp_0", "sp_1")
SP_DP = ("sp_0", "sp_1", "dp_0", "dp_1")
SP_SIZE = 16
DP_SIZE = 8
BLOCK = 512
SCALE = (PLAIN_HEAD_WIDTH + ROPE) ** (-0.5)
LOG2E = 1.4426950408889634

eps = 1e-06
rope_base = 10000.0
f32 = jnp.float32
bf16 = jnp.bfloat16


def pack_tables():
    first = np.zeros((384 + 256 + 128, 512), np.float32)
    second = np.zeros((384 + 256 + 128, 256), np.float32)
    for t in range(2):
        q, d, r = 192 * t, 384 + 128 * t, 640
        for c in range(64):
            first[q + c, 256 * t + c] = 1
            first[d + c, 256 * t + 64 + c] = 1
            second[q + 96 + c, 128 * t + c] = 1
            second[d + 64 + c, 128 * t + 64 + c] = 1
        for c in range(32):
            first[q + 64 + c, 256 * t + 128 + c] = 1
            first[q + 160 + c, 256 * t + 160 + c] = 1
            first[r + c, 256 * t + 192 + c] = 1
    return first, second


def unpack_tables():
    place = np.zeros((512, 384), np.float32)
    turn = np.zeros((512, 384), np.float32)
    for t in range(2):
        for h in range(2):
            row, col = 256 * t + 128 * h, 192 * t + 96 * h
            for c in range(96):
                place[row + c, col + c] = 1
            for c in range(64, 80):
                turn[row + c + 16, col + c] = 1
                turn[row + c, col + c + 16] = -1
    return place, turn


def rope_table():
    spread = np.zeros((128, 384), np.float32)
    for c in range(32):
        spread[c, c] = 1
        spread[32 + c, 128 + c] = 1
        spread[64 + c, 256 + c] = 1
    return spread


def turned_halves(x):
    lane = lax.broadcasted_iota(jnp.int32, x.shape, 1)
    return jnp.where(lane % 32 < 16, -pltpu.roll(x, 112, 1), pltpu.roll(x, 16, 1))


def pack_kernel(query, d_out, rope, first, second, cosine, sine, out):
    both = jnp.concatenate([query[...], d_out[...], rope[...]], axis=1)
    one = jnp.dot(both, first[...], preferred_element_type=f32)
    two = jnp.dot(both, second[...], preferred_element_type=f32).astype(bf16)
    for t in range(2):
        out[t, :, 0:128] = one[:, 256 * t : 256 * t + 128].astype(bf16)
        raw = one[:, 256 * t + 128 : 256 * t + 256]
        out[t, :, 128:256] = (raw * cosine[...] + turned_halves(raw) * sine[...]).astype(bf16)
        out[t, :, 256:384] = two[:, 128 * t : 128 * t + 128]


def pack(query, d_out, rope, cosine, sine):
    first, second = pack_tables()
    whole = lambda shape: pl.BlockSpec(shape, lambda j: (0, 0))
    return pl.pallas_call(
        pack_kernel,
        grid=(8,),
        in_specs=[
            pl.BlockSpec((TOKENS, 384), lambda j: (0, j)),
            pl.BlockSpec((TOKENS, 256), lambda j: (0, j)),
            whole((TOKENS, 128)),
            whole((768, 512)),
            whole((768, 256)),
            whole((TOKENS, 128)),
            whole((TOKENS, 128)),
        ],
        out_specs=pl.BlockSpec((2, TOKENS, 384), lambda j: (j, 0, 0)),
        out_shape=jax.ShapeDtypeStruct((SP_SIZE, TOKENS, 384), bf16),
        cost_estimate=pl.CostEstimate(
            flops=16 * 192 * 768 * 768, bytes_accessed=5_000_000, transcendentals=0
        ),
        name="pack",
    )(query, d_out, rope, jnp.asarray(first, bf16), jnp.asarray(second, bf16), cosine, sine)


def dot_t(a, b):
    return lax.dot_general(a, b, (((1,), (1,)), ((), ())), preferred_element_type=f32)


def lanes(x, combine):
    parts = [x[:, k : k + 128] for k in range(0, x.shape[1], 128)]
    return functools.reduce(combine, parts)


def attention_kernel(a_ref, q2_ref, kv_ref, k2_ref, out_ref, s_ref, dp_ref, m_ref, l_ref, d_ref, dq_ref, acc_ref):
    step = pl.program_id(0)
    count = LENGTH // BLOCK
    i = count - 1 - step

    @pl.when(step == 0)
    def _():
        acc_ref[...] = jnp.zeros_like(acc_ref)

    rows = pl.ds(pl.multiple_of(i * BLOCK, BLOCK), BLOCK)
    a = a_ref[rows, :]
    q2 = q2_ref[rows, :]
    lane = lax.broadcasted_iota(jnp.int32, (BLOCK, 128), 1)
    nope = jnp.where(lane < 64, a, jnp.zeros_like(a))
    cot = jnp.where(lane < 64, jnp.zeros_like(a), a)
    query = jnp.concatenate([nope, q2], axis=1)
    a_t = a.T
    q2_t = q2.T
    left_k = jnp.concatenate([q2_t[0:32], a_t[0:64]], axis=0)
    left_v = a_t[64:128]

    def tile(j):
        return pl.ds(pl.multiple_of(j * BLOCK, BLOCK), BLOCK)

    def key(j):
        return jnp.concatenate([kv_ref[tile(j), :], k2_ref[tile(j), :]], axis=1)

    m_ref[...] = jnp.full_like(m_ref, -1e30)
    l_ref[...] = jnp.zeros_like(l_ref)
    d_ref[...] = jnp.zeros_like(d_ref)
    dq_ref[...] = jnp.zeros_like(dq_ref)

    def scores(j, masked):
        s = dot_t(query, key(j))
        if masked:
            r = lax.broadcasted_iota(jnp.int32, (BLOCK, BLOCK), 0) // SPAN
            c = lax.broadcasted_iota(jnp.int32, (BLOCK, BLOCK), 1) // SPAN
            s = jnp.where(c <= r, s, -1e30)
        s_ref[:, tile(j)] = s
        m_ref[...] = jnp.maximum(m_ref[...], lanes(s, jnp.maximum))

    @pl.loop(0, i)
    def _(j):
        scores(j, False)

    scores(i, True)
    m = jnp.max(m_ref[...], axis=1, keepdims=True)

    def weights(j):
        dp = dot_t(cot, kv_ref[tile(j), :])
        e = jnp.exp2((s_ref[:, tile(j)] - m) * (SCALE * LOG2E))
        l_ref[...] += lanes(e, jnp.add)
        d_ref[...] += lanes(e * dp, jnp.add)
        s_ref[:, tile(j)] = e
        dp_ref[:, tile(j)] = dp

    @pl.loop(0, i + 1)
    def _(j):
        weights(j)

    inverse = 1.0 / jnp.sum(l_ref[...], axis=1, keepdims=True)
    delta = jnp.sum(d_ref[...], axis=1, keepdims=True) * inverse

    @pl.loop(0, i + 1)
    def _(j):
        p = s_ref[:, tile(j)] * inverse
        ds = (p * (dp_ref[:, tile(j)] - delta)).astype(bf16)
        dq_ref[...] += jnp.dot(ds, key(j), preferred_element_type=f32)
        acc_ref[0:96, tile(j)] += jnp.dot(left_k, ds, preferred_element_type=f32)
        acc_ref[96:160, tile(j)] += jnp.dot(left_v, p.astype(bf16), preferred_element_type=f32)

    dq = jnp.where(lane < 64, dq_ref[:, 0:128], pltpu.roll(dq_ref[:, 128:256], 64, 1)) * SCALE
    done = acc_ref[:, rows]
    k_rope = done[0:32] * SCALE
    k_nope = done[32:96] * SCALE
    low = jnp.concatenate([jnp.zeros((96, BLOCK), f32), k_rope], axis=0).T
    out_ref[:, 0:128] = jnp.where(lane < 96, dq, low).astype(bf16)
    out_ref[:, 128:256] = jnp.concatenate([k_nope, done[96:160]], axis=0).T.astype(bf16)


def attention(a, kv, ropes, head):
    count = LENGTH // BLOCK

    def column(k):
        return pl.BlockSpec((LENGTH, 128), lambda i: (0, k))

    return pl.pallas_call(
        attention_kernel,
        grid=(count,),
        in_specs=[column(2 * head), column(head), column(head), column(2)],
        out_specs=pl.BlockSpec((BLOCK, 256), lambda i: (count - 1 - i, 0)),
        out_shape=jax.ShapeDtypeStruct((LENGTH, 256), bf16),
        scratch_shapes=[
            pltpu.VMEM((BLOCK, LENGTH), f32),
            pltpu.VMEM((BLOCK, LENGTH), f32),
            pltpu.VMEM((BLOCK, 128), f32),
            pltpu.VMEM((BLOCK, 128), f32),
            pltpu.VMEM((BLOCK, 128), f32),
            pltpu.VMEM((BLOCK, 256), f32),
            pltpu.VMEM((160, LENGTH), f32),
        ],
        compiler_params=pltpu.CompilerParams(
            dimension_semantics=("arbitrary",), vmem_limit_bytes=48 * 1024 * 1024
        ),
        cost_estimate=pl.CostEstimate(
            flops=12_000_000_000, bytes_accessed=8_000_000, transcendentals=5_000_000
        ),
        name="attention",
    )(a, ropes, kv, ropes)


def finish_kernel(
    ret0, ret1, w, place, turn, latent, gain, wide_cos, wide_sin, cosine, sine,
    query_grad, latent_grad, rope_sum, acc,
):
    step = pl.program_id(0)

    @pl.when(step == 0)
    def _():
        acc[...] = jnp.zeros_like(acc)
        rope_sum[...] = jnp.zeros_like(rope_sum)

    left = [ret[t, :, 0:128] for t in range(2) for ret in (ret0, ret1)]
    row = jnp.concatenate(left, axis=1)
    plain = jnp.dot(row, place[...], preferred_element_type=f32)
    turned = jnp.dot(row, turn[...], preferred_element_type=f32)
    query_grad[...] = (plain * wide_cos[...] + turned * wide_sin[...]).astype(bf16)
    rope_sum[...] += sum(x.astype(f32) for x in left)
    total = acc[...]
    for t in range(2):
        right = jnp.concatenate([ret0[t, :, 128:256], ret1[t, :, 128:256]], axis=1)
        total += jnp.dot(right, w[t], preferred_element_type=f32)
    acc[...] = total

    @pl.when(step == pl.num_programs(0) - 1)
    def _():
        lat = latent[...].astype(f32)
        inverse = lax.rsqrt(jnp.mean(lat * lat, axis=1, keepdims=True) + eps)
        normed = lat * inverse
        scaled = acc[...] * gain[...]
        latent_grad[...] = inverse * (
            scaled - normed * jnp.mean(scaled * normed, axis=1, keepdims=True)
        )
        total_rope = rope_sum[...]
        rope_sum[...] = total_rope * cosine[...] - turned_halves(total_rope) * sine[...]


def finish(ret0, ret1, w, latent, gain, wide_cos, wide_sin, cosine, sine):
    fixed = lambda shape: pl.BlockSpec(shape, lambda j: (0,) * len(shape))
    place, turn = unpack_tables()
    return pl.pallas_call(
        finish_kernel,
        grid=(8,),
        in_specs=[
            pl.BlockSpec((2, TOKENS, 256), lambda j: (j, 0, 0)),
            pl.BlockSpec((2, TOKENS, 256), lambda j: (j, 0, 0)),
            pl.BlockSpec((2, 256, LATENT), lambda j: (j, 0, 0)),
            fixed((512, 384)),
            fixed((512, 384)),
            fixed((TOKENS, LATENT)),
            fixed((1, LATENT)),
            fixed((TOKENS, 384)),
            fixed((TOKENS, 384)),
            fixed((TOKENS, 128)),
            fixed((TOKENS, 128)),
        ],
        out_specs=[
            pl.BlockSpec((TOKENS, 384), lambda j: (0, j)),
            fixed((TOKENS, LATENT)),
            fixed((TOKENS, 128)),
        ],
        out_shape=[
            jax.ShapeDtypeStruct((TOKENS, 3072), bf16),
            jax.ShapeDtypeStruct((TOKENS, LATENT), f32),
            jax.ShapeDtypeStruct((TOKENS, 128), f32),
        ],
        scratch_shapes=[pltpu.VMEM((TOKENS, LATENT), f32)],
        compiler_params=pltpu.CompilerParams(dimension_semantics=("arbitrary",)),
        cost_estimate=pl.CostEstimate(
            flops=4_000_000_000, bytes_accessed=14_000_000, transcendentals=0
        ),
        name="finish",
    )(
        ret0, ret1, w, jnp.asarray(place, bf16), jnp.asarray(turn, bf16), latent, gain,
        wide_cos, wide_sin, cosine, sine,
    )


def inverse_frequency(index):
    return 1.0 / rope_base ** (2.0 * index.astype(f32) / ROPE)


def to_heads():
    pairs = []
    for i in range(DP_SIZE):
        for n in range(DP_SIZE):
            for b in range(2):
                pairs.append(((8 * b + n) * DP_SIZE + i, (2 * i + b) * DP_SIZE + n))
    return pairs


def place():
    z, y = lax.axis_index("sp_0"), lax.axis_index("sp_1")
    x, core = lax.axis_index("dp_0"), lax.axis_index("dp_1")
    return z, y, x, core


def on_sp(dz, dy):
    z, y, _, _ = place()
    return {"sp_0": lax.rem(z + dz, 4), "sp_1": lax.rem(y + dy, 4)}


def on_dp(dx, dcore):
    _, _, x, core = place()
    return {"dp_0": lax.rem(x + dx, 4), "dp_1": lax.rem(core + dcore, 2)}


SP_PEERS = [(k // 4, k % 4) for k in range(1, SP_SIZE)]
DP_PEERS = [(k // 2, k % 2) for k in range(1, DP_SIZE)]
NEAR = [(0, 1), (0, 3), (1, 0), (3, 0)]
X_PEERS = [(1, 0), (3, 0), (0, 1)]


def meet(sp_peers, dp_peers):
    barrier = pltpu.get_barrier_semaphore()
    for where in [on_sp(*p) for p in sp_peers] + [on_dp(*p) for p in dp_peers]:
        pl.semaphore_signal(
            barrier, inc=1, device_id=where, device_id_type=pl.DeviceIdType.MESH
        )
    pl.semaphore_wait(barrier, len(sp_peers) + len(dp_peers))


def copy_to(src, dst, send, recv, where):
    c = pltpu.make_async_remote_copy(
        src_ref=src,
        dst_ref=dst,
        send_sem=send,
        recv_sem=recv,
        device_id=where,
        device_id_type=pl.DeviceIdType.MESH,
    )
    c.start()
    return c


def keep(src, dst, sem):
    c = pltpu.make_async_copy(src, dst, sem)
    c.start()
    return c


def send_over_sp(block_for, got, send, recv):
    z, y, _, _ = place()
    sent = []
    for k, (dz, dy) in enumerate(SP_PEERS):
        there = 4 * lax.rem(z + dz, 4) + lax.rem(y + dy, 4)
        sent.append(
            copy_to(block_for(there), got.at[4 * z + y], send.at[k], recv.at[k], on_sp(dz, dy))
        )
    return sent


def send_over_dp(block_for, got, send, recv):
    _, _, x, core = place()
    sent = []
    for k, (dx, dcore) in enumerate(DP_PEERS):
        there = 2 * lax.rem(x + dx, 4) + lax.rem(core + dcore, 2)
        sent.append(
            copy_to(block_for(there), got.at[2 * x + core], send.at[k], recv.at[k], on_dp(dx, dcore))
        )
    return sent


def gather_over_sp(x, full, sems, between, midway=lambda: None):
    leg, leg_in, pass1, pass1_in, far, far_in, pass2, pass2_in = sems
    z, y, _, _ = place()
    me = 4 * z + y
    size = x.shape[0] // 2

    def along(h, s):
        return on_sp(0, s) if h == 0 else on_sp(s, 0)

    def across(h, s):
        return on_sp(s, 0) if h == 0 else on_sp(0, s)

    def block(h, s, c):
        dz, dy = (c, s) if h == 0 else (s, c)
        return 4 * lax.rem(z + dz, 4) + lax.rem(y + dy, 4)

    half = [pl.ds(h * size, size) for h in range(2)]
    quarter = [[pl.ds(h * size + q * size // 2, size // 2) for q in range(2)] for h in range(2)]
    ways = (1, 3)
    lines = (0, 3, 1, 2)
    first, second, third, fourth = {}, {}, {}, {}
    for w, s in enumerate(ways):
        for h in range(2):
            first[h, w] = copy_to(
                x.at[half[h]], full.at[me, half[h]], leg.at[h, w], leg_in.at[h, w], along(h, s)
            )
    for w, s in enumerate(ways):
        for h in range(2):
            third[h, 0, w] = copy_to(
                x.at[half[h]], full.at[me, half[h]], far.at[h, 0, w], far_in.at[h, 0, w], across(h, s)
            )
    rest = between()

    def onward(h, k):
        there = full.at[block(h, lines[k], 0), half[h]]
        for w, s in enumerate(ways):
            third[h, k, w] = copy_to(
                there, there, far.at[h, k, w], far_in.at[h, k, w], across(h, s)
            )

    for w, s in enumerate(ways):
        for h in range(2):
            first[h, w].wait_recv()
            piece = full.at[block(h, 4 - s, 0), quarter[h][w]]
            second[h, w] = copy_to(piece, piece, pass1.at[h, w], pass1_in.at[h, w], along(h, s))
            onward(h, w + 1)
    for h in range(2):
        for w in range(2):
            second[h, w].wait_recv()
        onward(h, 3)
    for k in range(4):
        if k == 2:
            midway()
        for w, s in enumerate(ways):
            for h in range(2):
                third[h, k, w].wait_recv()
                piece = full.at[block(h, lines[k], 4 - s), quarter[h][w]]
                fourth[h, k, w] = copy_to(
                    piece, piece, pass2.at[h, k, w], pass2_in.at[h, k, w], across(h, s)
                )
    for group in (first, second, third):
        for c in group.values():
            c.wait_send()
    for c in list(fourth.values()) + rest:
        c.wait()


def front_kernel(x, msgs, w, full, got, w_full, own_sem, *sems):
    msg_send, msg_recv, ring, ring_in, pair, pair_in = sems[8:]
    z, y, chip, core = place()
    me = 4 * z + y
    mine = 2 * chip + core
    size = w.shape[0] // 2
    meet(SP_PEERS, X_PEERS)
    ways = (1, 3)
    beside = {}

    def to_partner(k, source, where):
        beside[k] = copy_to(source, w_full.at[where], pair.at[k], pair_in.at[k], on_dp(0, 1))

    out = [
        copy_to(w, w_full.at[mine], ring.at[0, k], ring_in.at[0, k], on_dp(s, 0))
        for k, s in enumerate(ways)
    ]
    to_partner(0, w, mine)

    def between():
        own = [
            keep(x, full.at[me], own_sem.at[0]),
            keep(msgs.at[me], got.at[me], own_sem.at[1]),
            keep(w, w_full.at[mine], own_sem.at[2]),
        ]
        return own + send_over_sp(lambda there: msgs.at[there], got, msg_send, msg_recv)

    def row(s):
        return 2 * lax.rem(chip + s, 4) + core

    passed = []

    def midway():
        for k, s in enumerate(ways):
            out[k].wait_recv()
            piece = w_full.at[row(4 - s), pl.ds(k * size, size)]
            passed.append(copy_to(piece, piece, ring.at[1, k], ring_in.at[1, k], on_dp(s, 0)))
            to_partner(1 + k, w_full.at[row(4 - s)], row(4 - s))

    gather_over_sp(x, full, sems[:8], between, midway)
    for c in passed:
        c.wait_recv()
    to_partner(3, w_full.at[row(2)], row(2))
    for c in out + passed:
        c.wait_send()
    for c in beside.values():
        c.wait()


def tail_kernel(msgs, pieces, gain, got, arrived, gains, own_sem, *sems):
    z, y, chip, core = place()
    me = 4 * z + y
    mine = 2 * chip + core
    meet(SP_PEERS, DP_PEERS)
    going = send_over_dp(lambda there: pieces.at[there], arrived, sems[0], sems[1])
    going += send_over_sp(lambda there: gain, gains, sems[2], sems[3])
    going += send_over_sp(lambda there: msgs.at[there], got, sems[4], sems[5])
    going.append(keep(pieces.at[mine], arrived.at[mine], own_sem.at[0]))
    going.append(keep(gain, gains.at[me], own_sem.at[1]))
    going.append(keep(msgs.at[me], got.at[me], own_sem.at[2]))
    for c in going:
        c.wait()


def last_kernel(x, gain, full, gains, own_sem, *sems):
    z, y, chip, core = place()
    meet(NEAR, DP_PEERS)

    def between():
        own = [
            keep(x, full.at[4 * z + y], own_sem.at[0]),
            keep(gain, gains.at[2 * chip + core], own_sem.at[1]),
        ]
        return own + send_over_dp(lambda there: gain, gains, sems[8], sems[9])

    gather_over_sp(x, full, sems[:8], between)


def moving(kernel, collective_id, operands, results, sem_shapes):
    dma = pltpu.SemaphoreType.DMA
    return pl.pallas_call(
        kernel,
        in_specs=[pl.BlockSpec(memory_space=pltpu.VMEM)] * len(operands),
        out_specs=[pl.BlockSpec(memory_space=pl.ANY)] * len(results),
        out_shape=[jax.ShapeDtypeStruct(shape, dtype) for shape, dtype in results],
        scratch_shapes=[dma((3,))] + [dma(shape) for shape in sem_shapes for _ in range(2)],
        compiler_params=pltpu.CompilerParams(collective_id=collective_id, has_side_effects=True),
        cost_estimate=pl.CostEstimate(
            flops=8_000_000_000, bytes_accessed=8_000_000, transcendentals=0
        ),
    )(*operands)


GATHER_SEMS = [(2, 2), (2, 2), (2, 4, 2), (2, 4, 2)]


def exchange(value):
    return lax.all_to_all(value, SP, split_axis=0, concat_axis=0, tiled=True)


def layer(query, latent, rope_key, latent_norm_gain, key_up_matrix, value_up_matrix, out_grad):
    lat = latent[0].astype(f32)
    inv_rms = lax.rsqrt(jnp.mean(lat * lat, axis=-1, keepdims=True) + eps)
    nlat = (lat * inv_rms * latent_norm_gain).astype(bf16)

    shard = jnp.stack(
        [key_up_matrix.reshape(2, 2, 64, LATENT), value_up_matrix.reshape(2, 2, 64, LATENT)],
        axis=2,
    ).reshape(2, 256, LATENT)
    spot = lax.axis_index(SP)
    half = lax.dynamic_index_in_dim(shard, spot // 8, 0, keepdims=False)
    w_own = lax.ppermute(half, SP_DP, to_heads())

    position = (spot * TOKENS + jnp.arange(TOKENS)).astype(f32)[:, None]
    angle = position * inverse_frequency(jnp.arange(128) % 16)[None]
    cosine, sine = jnp.cos(angle), jnp.sin(angle)
    place = jnp.arange(384) % 96
    wide = position * jnp.where(place < 64, 0.0, inverse_frequency(place % 16))[None]
    wide_cos, wide_sin = jnp.cos(wide), jnp.sin(wide)

    rope_wide = jnp.pad(rope_key[0], ((0, 0), (0, 96)))
    sent = pack(query[0], out_grad[0], rope_wide, cosine, sine)
    nlat_full, got, w_whole = moving(
        front_kernel,
        0,
        [nlat, sent, shard.reshape(512, LATENT)],
        [
            ((SP_SIZE, TOKENS, LATENT), bf16),
            ((SP_SIZE, TOKENS, 384), bf16),
            ((DP_SIZE, 512, LATENT), bf16),
        ],
        GATHER_SEMS + [(SP_SIZE - 1,), (2, 2), (4,)],
    )
    nlat_full = nlat_full.reshape(LENGTH, LATENT)
    got = got.reshape(LENGTH, 384)
    w_whole = w_whole.reshape(SP_SIZE, 256, LATENT)

    ropes = jnp.dot(
        got[:, 128:256], jnp.asarray(rope_table(), bf16), preferred_element_type=f32
    ).astype(bf16)
    kv = lax.dot_general(
        nlat_full, w_own, (((1,), (1,)), ((), ())), preferred_element_type=f32
    ).astype(bf16)

    def weight_part(grads, h):
        d_w = lax.dot_general(
            grads[:, 128:256], nlat_full, (((0,), (0,)), ((), ())), preferred_element_type=f32
        )
        own = w_own[128 * h : 128 * h + 128].astype(f32)
        pieces = (
            d_w.reshape(2, DP_SIZE, 8, LATENT)
            .transpose(1, 0, 2, 3)
            .reshape(DP_SIZE, 16, LATENT)
        )
        return pieces, jnp.sum(d_w * own, axis=0)

    grads0 = attention(got, kv, ropes, 0)
    ret0 = exchange(grads0.reshape(SP_SIZE, TOKENS, 256))
    pieces0, gain0 = weight_part(grads0, 0)
    grads1 = attention(got, kv, ropes, 1)
    pieces1, gain1 = weight_part(grads1, 1)
    gain_part = ((gain0 + gain1) / latent_norm_gain).reshape(8, 128)
    ret1, arrived, gains = moving(
        tail_kernel,
        1,
        [
            grads1.reshape(SP_SIZE, TOKENS, 256),
            jnp.concatenate([pieces0, pieces1], axis=1),
            gain_part,
        ],
        [((SP_SIZE, TOKENS, 256), bf16), ((DP_SIZE, 32, LATENT), f32), ((SP_SIZE, 8, 128), f32)],
        [(DP_SIZE - 1,), (SP_SIZE - 1,), (SP_SIZE - 1,)],
    )
    moved = lax.ppermute(arrived.sum(axis=0), SP_DP, [(b, a) for a, b in to_heads()])
    blocks, gains = moving(
        last_kernel,
        2,
        [moved, gains.sum(axis=0)],
        [((SP_SIZE, 32, LATENT), f32), ((DP_SIZE, 8, 128), f32)],
        GATHER_SEMS + [(DP_SIZE - 1,)],
    )
    gain_grad = gains.sum(axis=0).reshape(LATENT)

    query_grad, latent_grad, rope_sum = finish(
        ret0, ret1, w_whole, latent[0], latent_norm_gain[None], wide_cos, wide_sin, cosine, sine
    )
    blocks = blocks.reshape(2, DP_SIZE, 2, 2, 8, LATENT).transpose(3, 0, 2, 1, 4, 5)
    blocks = blocks.reshape(2, 256, LATENT)
    return (
        query_grad[None],
        latent_grad[None],
        rope_sum[None, :, 96:128],
        blocks[0],
        blocks[1],
        gain_grad,
    )


def solution(mesh):
    split = Mesh(mesh.devices.reshape(4, 4, 4, 2), ("sp_0", "sp_1", "dp_0", "dp_1"))
    in_specs = (
        P(DP, SP, None),
        P(DP, SP, None),
        P(DP, SP, None),
        P(),
        P(DP, None),
        P(DP, None),
        P(DP, SP, None),
    )
    out_specs = (P(DP, SP, None), P(DP, SP, None), P(DP, SP, None), P(DP, None), P(DP, None), P())
    return jax.shard_map(layer, mesh=split, in_specs=in_specs, out_specs=out_specs, check_vma=False)
```

```python
import functools

import jax
import jax.numpy as jnp
import numpy as np
from jax import lax
from jax.experimental import pallas as pl
from jax.experimental.pallas import tpu as pltpu
from jax.sharding import Mesh
from jax.sharding import PartitionSpec as P


PLAIN_HEAD_WIDTH = 64
ROPE = 32
SPAN = 64
LATENT = 1024
LENGTH = 3072
TOKENS = 192
DP = ("dp_0", "dp_1")
SP = ("sp_0", "sp_1")
SP_DP = ("sp_0", "sp_1", "dp_0", "dp_1")
SP_SIZE = 16
DP_SIZE = 8
BLOCK = 512
SCALE = (PLAIN_HEAD_WIDTH + ROPE) ** (-0.5)
LOG2E = 1.4426950408889634

eps = 1e-06
rope_base = 10000.0
f32 = jnp.float32
bf16 = jnp.bfloat16


def pack_tables():
    first = np.zeros((384 + 256 + 128, 512), np.float32)
    second = np.zeros((384 + 256 + 128, 256), np.float32)
    for t in range(2):
        q, d, r = 192 * t, 384 + 128 * t, 640
        for c in range(64):
            first[q + c, 256 * t + c] = 1
            first[d + c, 256 * t + 64 + c] = 1
            second[q + 96 + c, 128 * t + c] = 1
            second[d + 64 + c, 128 * t + 64 + c] = 1
        for c in range(32):
            first[q + 64 + c, 256 * t + 128 + c] = 1
            first[q + 160 + c, 256 * t + 160 + c] = 1
            first[r + c, 256 * t + 192 + c] = 1
    return first, second


def unpack_tables():
    place = np.zeros((512, 384), np.float32)
    turn = np.zeros((512, 384), np.float32)
    for t in range(2):
        for h in range(2):
            row, col = 256 * t + 128 * h, 192 * t + 96 * h
            for c in range(96):
                place[row + c, col + c] = 1
            for c in range(64, 80):
                turn[row + c + 16, col + c] = 1
                turn[row + c, col + c + 16] = -1
    return place, turn


def rope_table():
    spread = np.zeros((128, 384), np.float32)
    for c in range(32):
        spread[c, c] = 1
        spread[32 + c, 128 + c] = 1
        spread[64 + c, 256 + c] = 1
    return spread


def turned_halves(x):
    lane = lax.broadcasted_iota(jnp.int32, x.shape, 1)
    return jnp.where(lane % 32 < 16, -pltpu.roll(x, 112, 1), pltpu.roll(x, 16, 1))


def pack_kernel(query, d_out, rope, first, second, cosine, sine, out):
    both = jnp.concatenate([query[...], d_out[...], rope[...]], axis=1)
    one = jnp.dot(both, first[...], preferred_element_type=f32)
    two = jnp.dot(both, second[...], preferred_element_type=f32).astype(bf16)
    for t in range(2):
        out[t, :, 0:128] = one[:, 256 * t : 256 * t + 128].astype(bf16)
        raw = one[:, 256 * t + 128 : 256 * t + 256]
        out[t, :, 128:256] = (raw * cosine[...] + turned_halves(raw) * sine[...]).astype(bf16)
        out[t, :, 256:384] = two[:, 128 * t : 128 * t + 128]


def pack(query, d_out, rope, cosine, sine):
    first, second = pack_tables()
    whole = lambda shape: pl.BlockSpec(shape, lambda j: (0, 0))
    return pl.pallas_call(
        pack_kernel,
        grid=(8,),
        in_specs=[
            pl.BlockSpec((TOKENS, 384), lambda j: (0, j)),
            pl.BlockSpec((TOKENS, 256), lambda j: (0, j)),
            whole((TOKENS, 128)),
            whole((768, 512)),
            whole((768, 256)),
            whole((TOKENS, 128)),
            whole((TOKENS, 128)),
        ],
        out_specs=pl.BlockSpec((2, TOKENS, 384), lambda j: (j, 0, 0)),
        out_shape=jax.ShapeDtypeStruct((SP_SIZE, TOKENS, 384), bf16),
        cost_estimate=pl.CostEstimate(
            flops=16 * 192 * 768 * 768, bytes_accessed=5_000_000, transcendentals=0
        ),
        name="pack",
    )(query, d_out, rope, jnp.asarray(first, bf16), jnp.asarray(second, bf16), cosine, sine)


def dot_t(a, b):
    return lax.dot_general(a, b, (((1,), (1,)), ((), ())), preferred_element_type=f32)


def lanes(x, combine):
    parts = [x[:, k : k + 128] for k in range(0, x.shape[1], 128)]
    return functools.reduce(combine, parts)


def attention_kernel(a_ref, q2_ref, kv_ref, k2_ref, out_ref, s_ref, dp_ref, m_ref, l_ref, d_ref, dq_ref, acc_ref):
    step = pl.program_id(0)
    count = LENGTH // BLOCK
    i = count - 1 - step

    @pl.when(step == 0)
    def _():
        acc_ref[...] = jnp.zeros_like(acc_ref)

    rows = pl.ds(pl.multiple_of(i * BLOCK, BLOCK), BLOCK)
    a = a_ref[rows, :]
    q2 = q2_ref[rows, :]
    lane = lax.broadcasted_iota(jnp.int32, (BLOCK, 128), 1)
    nope = jnp.where(lane < 64, a, jnp.zeros_like(a))
    cot = jnp.where(lane < 64, jnp.zeros_like(a), a)
    query = jnp.concatenate([nope, q2], axis=1)
    a_t = a.T
    q2_t = q2.T
    left_k = jnp.concatenate([q2_t[0:32], a_t[0:64]], axis=0)
    left_v = a_t[64:128]

    def tile(j):
        return pl.ds(pl.multiple_of(j * BLOCK, BLOCK), BLOCK)

    def key(j):
        return jnp.concatenate([kv_ref[tile(j), :], k2_ref[tile(j), :]], axis=1)

    m_ref[...] = jnp.full_like(m_ref, -1e30)
    l_ref[...] = jnp.zeros_like(l_ref)
    d_ref[...] = jnp.zeros_like(d_ref)
    dq_ref[...] = jnp.zeros_like(dq_ref)

    def scores(j, masked):
        s = dot_t(query, key(j))
        if masked:
            r = lax.broadcasted_iota(jnp.int32, (BLOCK, BLOCK), 0) // SPAN
            c = lax.broadcasted_iota(jnp.int32, (BLOCK, BLOCK), 1) // SPAN
            s = jnp.where(c <= r, s, -1e30)
        s_ref[:, tile(j)] = s
        m_ref[...] = jnp.maximum(m_ref[...], lanes(s, jnp.maximum))

    @pl.loop(0, i)
    def _(j):
        scores(j, False)

    scores(i, True)
    m = jnp.max(m_ref[...], axis=1, keepdims=True)

    def weights(j):
        dp = dot_t(cot, kv_ref[tile(j), :])
        e = jnp.exp2((s_ref[:, tile(j)] - m) * (SCALE * LOG2E))
        l_ref[...] += lanes(e, jnp.add)
        d_ref[...] += lanes(e * dp, jnp.add)
        s_ref[:, tile(j)] = e
        dp_ref[:, tile(j)] = dp

    @pl.loop(0, i + 1)
    def _(j):
        weights(j)

    inverse = 1.0 / jnp.sum(l_ref[...], axis=1, keepdims=True)
    delta = jnp.sum(d_ref[...], axis=1, keepdims=True) * inverse

    @pl.loop(0, i + 1)
    def _(j):
        p = s_ref[:, tile(j)] * inverse
        ds = (p * (dp_ref[:, tile(j)] - delta)).astype(bf16)
        dq_ref[...] += jnp.dot(ds, key(j), preferred_element_type=f32)
        acc_ref[0:96, tile(j)] += jnp.dot(left_k, ds, preferred_element_type=f32)
        acc_ref[96:160, tile(j)] += jnp.dot(left_v, p.astype(bf16), preferred_element_type=f32)

    dq = jnp.where(lane < 64, dq_ref[:, 0:128], pltpu.roll(dq_ref[:, 128:256], 64, 1)) * SCALE
    done = acc_ref[:, rows]
    k_rope = done[0:32] * SCALE
    k_nope = done[32:96] * SCALE
    low = jnp.concatenate([jnp.zeros((96, BLOCK), f32), k_rope], axis=0).T
    out_ref[:, 0:128] = jnp.where(lane < 96, dq, low).astype(bf16)
    out_ref[:, 128:256] = jnp.concatenate([k_nope, done[96:160]], axis=0).T.astype(bf16)


def attention(a, kv, ropes, head):
    count = LENGTH // BLOCK

    def column(k):
        return pl.BlockSpec((LENGTH, 128), lambda i: (0, k))

    return pl.pallas_call(
        attention_kernel,
        grid=(count,),
        in_specs=[column(2 * head), column(head), column(head), column(2)],
        out_specs=pl.BlockSpec((BLOCK, 256), lambda i: (count - 1 - i, 0)),
        out_shape=jax.ShapeDtypeStruct((LENGTH, 256), bf16),
        scratch_shapes=[
            pltpu.VMEM((BLOCK, LENGTH), f32),
            pltpu.VMEM((BLOCK, LENGTH), f32),
            pltpu.VMEM((BLOCK, 128), f32),
            pltpu.VMEM((BLOCK, 128), f32),
            pltpu.VMEM((BLOCK, 128), f32),
            pltpu.VMEM((BLOCK, 256), f32),
            pltpu.VMEM((160, LENGTH), f32),
        ],
        compiler_params=pltpu.CompilerParams(
            dimension_semantics=("arbitrary",), vmem_limit_bytes=48 * 1024 * 1024
        ),
        cost_estimate=pl.CostEstimate(
            flops=12_000_000_000, bytes_accessed=8_000_000, transcendentals=5_000_000
        ),
        name="attention",
    )(a, ropes, kv, ropes)


def finish_kernel(
    ret0, ret1, w, place, turn, latent, gain, wide_cos, wide_sin, cosine, sine,
    query_grad, latent_grad, rope_sum, acc,
):
    step = pl.program_id(0)

    @pl.when(step == 0)
    def _():
        acc[...] = jnp.zeros_like(acc)
        rope_sum[...] = jnp.zeros_like(rope_sum)

    left = [ret[t, :, 0:128] for t in range(2) for ret in (ret0, ret1)]
    row = jnp.concatenate(left, axis=1)
    plain = jnp.dot(row, place[...], preferred_element_type=f32)
    turned = jnp.dot(row, turn[...], preferred_element_type=f32)
    query_grad[...] = (plain * wide_cos[...] + turned * wide_sin[...]).astype(bf16)
    rope_sum[...] += sum(x.astype(f32) for x in left)
    total = acc[...]
    for t in range(2):
        right = jnp.concatenate([ret0[t, :, 128:256], ret1[t, :, 128:256]], axis=1)
        total += jnp.dot(right, w[t], preferred_element_type=f32)
    acc[...] = total

    @pl.when(step == pl.num_programs(0) - 1)
    def _():
        lat = latent[...].astype(f32)
        inverse = lax.rsqrt(jnp.mean(lat * lat, axis=1, keepdims=True) + eps)
        normed = lat * inverse
        scaled = acc[...] * gain[...]
        latent_grad[...] = inverse * (
            scaled - normed * jnp.mean(scaled * normed, axis=1, keepdims=True)
        )
        total_rope = rope_sum[...]
        rope_sum[...] = total_rope * cosine[...] - turned_halves(total_rope) * sine[...]


def finish(ret0, ret1, w, latent, gain, wide_cos, wide_sin, cosine, sine):
    fixed = lambda shape: pl.BlockSpec(shape, lambda j: (0,) * len(shape))
    place, turn = unpack_tables()
    return pl.pallas_call(
        finish_kernel,
        grid=(8,),
        in_specs=[
            pl.BlockSpec((2, TOKENS, 256), lambda j: (j, 0, 0)),
            pl.BlockSpec((2, TOKENS, 256), lambda j: (j, 0, 0)),
            pl.BlockSpec((2, 256, LATENT), lambda j: (j, 0, 0)),
            fixed((512, 384)),
            fixed((512, 384)),
            fixed((TOKENS, LATENT)),
            fixed((1, LATENT)),
            fixed((TOKENS, 384)),
            fixed((TOKENS, 384)),
            fixed((TOKENS, 128)),
            fixed((TOKENS, 128)),
        ],
        out_specs=[
            pl.BlockSpec((TOKENS, 384), lambda j: (0, j)),
            fixed((TOKENS, LATENT)),
            fixed((TOKENS, 128)),
        ],
        out_shape=[
            jax.ShapeDtypeStruct((TOKENS, 3072), bf16),
            jax.ShapeDtypeStruct((TOKENS, LATENT), f32),
            jax.ShapeDtypeStruct((TOKENS, 128), f32),
        ],
        scratch_shapes=[pltpu.VMEM((TOKENS, LATENT), f32)],
        compiler_params=pltpu.CompilerParams(dimension_semantics=("arbitrary",)),
        cost_estimate=pl.CostEstimate(
            flops=4_000_000_000, bytes_accessed=14_000_000, transcendentals=0
        ),
        name="finish",
    )(
        ret0, ret1, w, jnp.asarray(place, bf16), jnp.asarray(turn, bf16), latent, gain,
        wide_cos, wide_sin, cosine, sine,
    )


def inverse_frequency(index):
    return 1.0 / rope_base ** (2.0 * index.astype(f32) / ROPE)


def to_heads():
    pairs = []
    for i in range(DP_SIZE):
        for n in range(DP_SIZE):
            for b in range(2):
                pairs.append(((8 * b + n) * DP_SIZE + i, (2 * i + b) * DP_SIZE + n))
    return pairs


def place():
    z, y = lax.axis_index("sp_0"), lax.axis_index("sp_1")
    x, core = lax.axis_index("dp_0"), lax.axis_index("dp_1")
    return z, y, x, core


def on_sp(dz, dy):
    z, y, _, _ = place()
    return {"sp_0": lax.rem(z + dz, 4), "sp_1": lax.rem(y + dy, 4)}


def on_dp(dx, dcore):
    _, _, x, core = place()
    return {"dp_0": lax.rem(x + dx, 4), "dp_1": lax.rem(core + dcore, 2)}


SP_PEERS = [(k // 4, k % 4) for k in range(1, SP_SIZE)]
DP_PEERS = [(k // 2, k % 2) for k in range(1, DP_SIZE)]
NEAR = [(0, 1), (0, 3), (1, 0), (3, 0)]
X_PEERS = [(1, 0), (3, 0), (0, 1)]


def meet(sp_peers, dp_peers):
    barrier = pltpu.get_barrier_semaphore()
    for where in [on_sp(*p) for p in sp_peers] + [on_dp(*p) for p in dp_peers]:
        pl.semaphore_signal(
            barrier, inc=1, device_id=where, device_id_type=pl.DeviceIdType.MESH
        )
    pl.semaphore_wait(barrier, len(sp_peers) + len(dp_peers))


def copy_to(src, dst, send, recv, where):
    c = pltpu.make_async_remote_copy(
        src_ref=src,
        dst_ref=dst,
        send_sem=send,
        recv_sem=recv,
        device_id=where,
        device_id_type=pl.DeviceIdType.MESH,
    )
    c.start()
    return c


def keep(src, dst, sem):
    c = pltpu.make_async_copy(src, dst, sem)
    c.start()
    return c


def send_over_sp(block_for, got, send, recv):
    z, y, _, _ = place()
    sent = []
    for k, (dz, dy) in enumerate(SP_PEERS):
        there = 4 * lax.rem(z + dz, 4) + lax.rem(y + dy, 4)
        sent.append(
            copy_to(block_for(there), got.at[4 * z + y], send.at[k], recv.at[k], on_sp(dz, dy))
        )
    return sent


RELAYED = {
    (2, 0): ((3, 0), (3, 0)),
    (2, 1): ((3, 1), (3, 0)),
    (0, 2): ((0, 3), (0, 3)),
    (1, 2): ((1, 3), (0, 3)),
}


def send_balanced(msgs, got, held, send, recv, leg_send, leg_recv):
    z, y, _, _ = place()

    def number(dz, dy):
        return 4 * lax.rem(z + dz, 4) + lax.rem(y + dy, 4)

    legs = []
    for r, (goal, (leg, _)) in enumerate(RELAYED.items()):
        legs.append(
            copy_to(msgs.at[number(*goal)], held.at[r], leg_send.at[r], leg_recv.at[r], on_sp(*leg))
        )
    sent = []
    for k, peer in enumerate(SP_PEERS):
        if peer not in RELAYED:
            sent.append(
                copy_to(
                    msgs.at[number(*peer)], got.at[number(0, 0)], send.at[k], recv.at[k], on_sp(*peer)
                )
            )

    def pass_on():
        passed = []
        for r, (goal, (leg, step)) in enumerate(RELAYED.items()):
            legs[r].wait_recv()
            source = number((4 - leg[0]) % 4, (4 - leg[1]) % 4)
            k = SP_PEERS.index(goal)
            passed.append(
                copy_to(held.at[r], got.at[source], send.at[k], recv.at[k], on_sp(*step))
            )
        for c in legs:
            c.wait_send()
        return passed

    return sent, pass_on


def send_over_dp(block_for, got, send, recv):
    _, _, x, core = place()
    sent = []
    for k, (dx, dcore) in enumerate(DP_PEERS):
        there = 2 * lax.rem(x + dx, 4) + lax.rem(core + dcore, 2)
        sent.append(
            copy_to(block_for(there), got.at[2 * x + core], send.at[k], recv.at[k], on_dp(dx, dcore))
        )
    return sent


def gather_over_sp(x, full, sems, between, midway=lambda: None):
    leg, leg_in, pass1, pass1_in, far, far_in, pass2, pass2_in = sems
    z, y, _, _ = place()
    me = 4 * z + y
    size = x.shape[0] // 2

    def along(h, s):
        return on_sp(0, s) if h == 0 else on_sp(s, 0)

    def across(h, s):
        return on_sp(s, 0) if h == 0 else on_sp(0, s)

    def block(h, s, c):
        dz, dy = (c, s) if h == 0 else (s, c)
        return 4 * lax.rem(z + dz, 4) + lax.rem(y + dy, 4)

    half = [pl.ds(h * size, size) for h in range(2)]
    quarter = [[pl.ds(h * size + q * size // 2, size // 2) for q in range(2)] for h in range(2)]
    ways = (1, 3)
    lines = (0, 3, 1, 2)
    first, second, third, fourth = {}, {}, {}, {}
    for w, s in enumerate(ways):
        for h in range(2):
            first[h, w] = copy_to(
                x.at[half[h]], full.at[me, half[h]], leg.at[h, w], leg_in.at[h, w], along(h, s)
            )
    for w, s in enumerate(ways):
        for h in range(2):
            third[h, 0, w] = copy_to(
                x.at[half[h]], full.at[me, half[h]], far.at[h, 0, w], far_in.at[h, 0, w], across(h, s)
            )
    rest = between()

    def onward(h, k):
        there = full.at[block(h, lines[k], 0), half[h]]
        for w, s in enumerate(ways):
            third[h, k, w] = copy_to(
                there, there, far.at[h, k, w], far_in.at[h, k, w], across(h, s)
            )

    for w, s in enumerate(ways):
        for h in range(2):
            first[h, w].wait_recv()
            piece = full.at[block(h, 4 - s, 0), quarter[h][w]]
            second[h, w] = copy_to(piece, piece, pass1.at[h, w], pass1_in.at[h, w], along(h, s))
            onward(h, w + 1)
    for h in range(2):
        for w in range(2):
            second[h, w].wait_recv()
        onward(h, 3)
    for k in range(4):
        if k == 2:
            midway()
        for w, s in enumerate(ways):
            for h in range(2):
                third[h, k, w].wait_recv()
                piece = full.at[block(h, lines[k], 4 - s), quarter[h][w]]
                fourth[h, k, w] = copy_to(
                    piece, piece, pass2.at[h, k, w], pass2_in.at[h, k, w], across(h, s)
                )
    for group in (first, second, third):
        for c in group.values():
            c.wait_send()
    for c in list(fourth.values()) + rest:
        c.wait()


def front_kernel(x, msgs, w, full, got, w_full, held, own_sem, *sems):
    msg_send, msg_recv, ring, ring_in, pair, pair_in, leg_send, leg_recv = sems[8:]
    later = []
    z, y, chip, core = place()
    me = 4 * z + y
    mine = 2 * chip + core
    size = w.shape[0] // 2
    meet(SP_PEERS, X_PEERS)
    ways = (1, 3)
    beside = {}

    def to_partner(k, source, where):
        beside[k] = copy_to(source, w_full.at[where], pair.at[k], pair_in.at[k], on_dp(0, 1))

    out = [
        copy_to(w, w_full.at[mine], ring.at[0, k], ring_in.at[0, k], on_dp(s, 0))
        for k, s in enumerate(ways)
    ]
    to_partner(0, w, mine)

    def between():
        own = [
            keep(x, full.at[me], own_sem.at[0]),
            keep(msgs.at[me], got.at[me], own_sem.at[1]),
            keep(w, w_full.at[mine], own_sem.at[2]),
        ]
        sent, pass_on = send_balanced(msgs, got, held, msg_send, msg_recv, leg_send, leg_recv)
        later.append(pass_on)
        return own + sent

    def row(s):
        return 2 * lax.rem(chip + s, 4) + core

    passed = []

    def midway():
        out.extend(later[0]())
        for k, s in enumerate(ways):
            out[k].wait_recv()
            piece = w_full.at[row(4 - s), pl.ds(k * size, size)]
            passed.append(copy_to(piece, piece, ring.at[1, k], ring_in.at[1, k], on_dp(s, 0)))
            to_partner(1 + k, w_full.at[row(4 - s)], row(4 - s))

    gather_over_sp(x, full, sems[:8], between, midway)
    for c in passed:
        c.wait_recv()
    to_partner(3, w_full.at[row(2)], row(2))
    for c in out[:2] + passed:
        c.wait_send()
    for c in out[2:]:
        c.wait()
    for c in beside.values():
        c.wait()


def tail_kernel(msgs, pieces, gain, got, arrived, gains, held, own_sem, *sems):
    z, y, chip, core = place()
    me = 4 * z + y
    mine = 2 * chip + core
    meet(SP_PEERS, DP_PEERS)
    going, pass_on = send_balanced(msgs, got, held, *sems[4:8])
    going += send_over_dp(lambda there: pieces.at[there], arrived, sems[0], sems[1])
    going += send_over_sp(lambda there: gain, gains, sems[2], sems[3])
    going.append(keep(pieces.at[mine], arrived.at[mine], own_sem.at[0]))
    going.append(keep(gain, gains.at[me], own_sem.at[1]))
    going.append(keep(msgs.at[me], got.at[me], own_sem.at[2]))
    going += pass_on()
    for c in going:
        c.wait()


def last_kernel(x, gain, full, gains, own_sem, *sems):
    z, y, chip, core = place()
    meet(NEAR, DP_PEERS)

    def between():
        own = [
            keep(x, full.at[4 * z + y], own_sem.at[0]),
            keep(gain, gains.at[2 * chip + core], own_sem.at[1]),
        ]
        return own + send_over_dp(lambda there: gain, gains, sems[8], sems[9])

    gather_over_sp(x, full, sems[:8], between)


def moving(kernel, collective_id, operands, results, sem_shapes):
    dma = pltpu.SemaphoreType.DMA
    return pl.pallas_call(
        kernel,
        in_specs=[pl.BlockSpec(memory_space=pltpu.VMEM)] * len(operands),
        out_specs=[pl.BlockSpec(memory_space=pl.ANY)] * len(results),
        out_shape=[jax.ShapeDtypeStruct(shape, dtype) for shape, dtype in results],
        scratch_shapes=[dma((3,))] + [dma(shape) for shape in sem_shapes for _ in range(2)],
        compiler_params=pltpu.CompilerParams(collective_id=collective_id, has_side_effects=True),
        cost_estimate=pl.CostEstimate(
            flops=8_000_000_000, bytes_accessed=8_000_000, transcendentals=0
        ),
    )(*operands)


GATHER_SEMS = [(2, 2), (2, 2), (2, 4, 2), (2, 4, 2)]


def exchange(value):
    return lax.all_to_all(value, SP, split_axis=0, concat_axis=0, tiled=True)


def layer(query, latent, rope_key, latent_norm_gain, key_up_matrix, value_up_matrix, out_grad):
    lat = latent[0].astype(f32)
    inv_rms = lax.rsqrt(jnp.mean(lat * lat, axis=-1, keepdims=True) + eps)
    nlat = (lat * inv_rms * latent_norm_gain).astype(bf16)

    shard = jnp.stack(
        [key_up_matrix.reshape(2, 2, 64, LATENT), value_up_matrix.reshape(2, 2, 64, LATENT)],
        axis=2,
    ).reshape(2, 256, LATENT)
    spot = lax.axis_index(SP)
    half = lax.dynamic_index_in_dim(shard, spot // 8, 0, keepdims=False)
    w_own = lax.ppermute(half, SP_DP, to_heads())

    position = (spot * TOKENS + jnp.arange(TOKENS)).astype(f32)[:, None]
    angle = position * inverse_frequency(jnp.arange(128) % 16)[None]
    cosine, sine = jnp.cos(angle), jnp.sin(angle)
    place = jnp.arange(384) % 96
    wide = position * jnp.where(place < 64, 0.0, inverse_frequency(place % 16))[None]
    wide_cos, wide_sin = jnp.cos(wide), jnp.sin(wide)

    rope_wide = jnp.pad(rope_key[0], ((0, 0), (0, 96)))
    sent = pack(query[0], out_grad[0], rope_wide, cosine, sine)
    nlat_full, got, w_whole, _ = moving(
        front_kernel,
        0,
        [nlat, sent, shard.reshape(512, LATENT)],
        [
            ((SP_SIZE, TOKENS, LATENT), bf16),
            ((SP_SIZE, TOKENS, 384), bf16),
            ((DP_SIZE, 512, LATENT), bf16),
            ((len(RELAYED), TOKENS, 384), bf16),
        ],
        GATHER_SEMS + [(SP_SIZE - 1,), (2, 2), (4,), (len(RELAYED),)],
    )
    nlat_full = nlat_full.reshape(LENGTH, LATENT)
    got = got.reshape(LENGTH, 384)
    w_whole = w_whole.reshape(SP_SIZE, 256, LATENT)

    ropes = jnp.dot(
        got[:, 128:256], jnp.asarray(rope_table(), bf16), preferred_element_type=f32
    ).astype(bf16)
    kv = lax.dot_general(
        nlat_full, w_own, (((1,), (1,)), ((), ())), preferred_element_type=f32
    ).astype(bf16)

    def weight_part(grads, h):
        d_w = lax.dot_general(
            grads[:, 128:256], nlat_full, (((0,), (0,)), ((), ())), preferred_element_type=f32
        )
        own = w_own[128 * h : 128 * h + 128].astype(f32)
        pieces = (
            d_w.reshape(2, DP_SIZE, 8, LATENT)
            .transpose(1, 0, 2, 3)
            .reshape(DP_SIZE, 16, LATENT)
        )
        return pieces, jnp.sum(d_w * own, axis=0)

    grads0 = attention(got, kv, ropes, 0)
    ret0 = exchange(grads0.reshape(SP_SIZE, TOKENS, 256))
    pieces0, gain0 = weight_part(grads0, 0)
    grads1 = attention(got, kv, ropes, 1)
    pieces1, gain1 = weight_part(grads1, 1)
    gain_part = ((gain0 + gain1) / latent_norm_gain).reshape(8, 128)
    ret1, arrived, gains, _ = moving(
        tail_kernel,
        1,
        [
            grads1.reshape(SP_SIZE, TOKENS, 256),
            jnp.concatenate([pieces0, pieces1], axis=1),
            gain_part,
        ],
        [
            ((SP_SIZE, TOKENS, 256), bf16),
            ((DP_SIZE, 32, LATENT), f32),
            ((SP_SIZE, 8, 128), f32),
            ((len(RELAYED), TOKENS, 256), bf16),
        ],
        [(DP_SIZE - 1,), (SP_SIZE - 1,), (SP_SIZE - 1,), (len(RELAYED),)],
    )
    moved = lax.ppermute(arrived.sum(axis=0), SP_DP, [(b, a) for a, b in to_heads()])
    blocks, gains = moving(
        last_kernel,
        2,
        [moved, gains.sum(axis=0)],
        [((SP_SIZE, 32, LATENT), f32), ((DP_SIZE, 8, 128), f32)],
        GATHER_SEMS + [(DP_SIZE - 1,)],
    )
    gain_grad = gains.sum(axis=0).reshape(LATENT)

    query_grad, latent_grad, rope_sum = finish(
        ret0, ret1, w_whole, latent[0], latent_norm_gain[None], wide_cos, wide_sin, cosine, sine
    )
    blocks = blocks.reshape(2, DP_SIZE, 2, 2, 8, LATENT).transpose(3, 0, 2, 1, 4, 5)
    blocks = blocks.reshape(2, 256, LATENT)
    return (
        query_grad[None],
        latent_grad[None],
        rope_sum[None, :, 96:128],
        blocks[0],
        blocks[1],
        gain_grad,
    )


def solution(mesh):
    split = Mesh(mesh.devices.reshape(4, 4, 4, 2), ("sp_0", "sp_1", "dp_0", "dp_1"))
    in_specs = (
        P(DP, SP, None),
        P(DP, SP, None),
        P(DP, SP, None),
        P(),
        P(DP, None),
        P(DP, None),
        P(DP, SP, None),
    )
    out_specs = (P(DP, SP, None), P(DP, SP, None), P(DP, SP, None), P(DP, None), P(DP, None), P())
    return jax.shard_map(layer, mesh=split, in_specs=in_specs, out_specs=out_specs, check_vma=False)
```

```python
import functools

import jax
import jax.numpy as jnp
import numpy as np
from jax import lax
from jax.experimental import pallas as pl
from jax.experimental.pallas import tpu as pltpu
from jax.sharding import Mesh
from jax.sharding import PartitionSpec as P


PLAIN_HEAD_WIDTH = 64
ROPE = 32
SPAN = 64
LATENT = 1024
LENGTH = 3072
TOKENS = 192
DP = ("dp_0", "dp_1")
SP = ("sp_0", "sp_1")
SP_DP = ("sp_0", "sp_1", "dp_0", "dp_1")
SP_SIZE = 16
DP_SIZE = 8
BLOCK = 512
SCALE = (PLAIN_HEAD_WIDTH + ROPE) ** (-0.5)
LOG2E = 1.4426950408889634

eps = 1e-06
rope_base = 10000.0
f32 = jnp.float32
bf16 = jnp.bfloat16


def pack_tables():
    first = np.zeros((384 + 256 + 128, 512), np.float32)
    second = np.zeros((384 + 256 + 128, 256), np.float32)
    for t in range(2):
        q, d, r = 192 * t, 384 + 128 * t, 640
        for c in range(64):
            first[q + c, 256 * t + c] = 1
            first[d + c, 256 * t + 64 + c] = 1
            second[q + 96 + c, 128 * t + c] = 1
            second[d + 64 + c, 128 * t + 64 + c] = 1
        for c in range(32):
            first[q + 64 + c, 256 * t + 128 + c] = 1
            first[q + 160 + c, 256 * t + 160 + c] = 1
            first[r + c, 256 * t + 192 + c] = 1
    return first, second


def unpack_tables():
    place = np.zeros((512, 384), np.float32)
    turn = np.zeros((512, 384), np.float32)
    for t in range(2):
        for h in range(2):
            row, col = 256 * t + 128 * h, 192 * t + 96 * h
            for c in range(96):
                place[row + c, col + c] = 1
            for c in range(64, 80):
                turn[row + c + 16, col + c] = 1
                turn[row + c, col + c + 16] = -1
    return place, turn


def rope_table():
    spread = np.zeros((128, 384), np.float32)
    for c in range(32):
        spread[c, c] = 1
        spread[32 + c, 128 + c] = 1
        spread[64 + c, 256 + c] = 1
    return spread


def turned_halves(x):
    lane = lax.broadcasted_iota(jnp.int32, x.shape, 1)
    return jnp.where(lane % 32 < 16, -pltpu.roll(x, 112, 1), pltpu.roll(x, 16, 1))


def pack_kernel(query, d_out, rope, first, second, cosine, sine, out):
    both = jnp.concatenate([query[...], d_out[...], rope[...]], axis=1)
    one = jnp.dot(both, first[...], preferred_element_type=f32)
    two = jnp.dot(both, second[...], preferred_element_type=f32).astype(bf16)
    for t in range(2):
        out[t, :, 0:128] = one[:, 256 * t : 256 * t + 128].astype(bf16)
        raw = one[:, 256 * t + 128 : 256 * t + 256]
        out[t, :, 128:256] = (raw * cosine[...] + turned_halves(raw) * sine[...]).astype(bf16)
        out[t, :, 256:384] = two[:, 128 * t : 128 * t + 128]


def pack(query, d_out, rope, cosine, sine):
    first, second = pack_tables()
    whole = lambda shape: pl.BlockSpec(shape, lambda j: (0, 0))
    return pl.pallas_call(
        pack_kernel,
        grid=(8,),
        in_specs=[
            pl.BlockSpec((TOKENS, 384), lambda j: (0, j)),
            pl.BlockSpec((TOKENS, 256), lambda j: (0, j)),
            whole((TOKENS, 128)),
            whole((768, 512)),
            whole((768, 256)),
            whole((TOKENS, 128)),
            whole((TOKENS, 128)),
        ],
        out_specs=pl.BlockSpec((2, TOKENS, 384), lambda j: (j, 0, 0)),
        out_shape=jax.ShapeDtypeStruct((SP_SIZE, TOKENS, 384), bf16),
        cost_estimate=pl.CostEstimate(
            flops=16 * 192 * 768 * 768, bytes_accessed=5_000_000, transcendentals=0
        ),
        name="pack",
    )(query, d_out, rope, jnp.asarray(first, bf16), jnp.asarray(second, bf16), cosine, sine)


def dot_t(a, b):
    return lax.dot_general(a, b, (((1,), (1,)), ((), ())), preferred_element_type=f32)


def lanes(x, combine):
    parts = [x[:, k : k + 128] for k in range(0, x.shape[1], 128)]
    return functools.reduce(combine, parts)


def attention_kernel(a_ref, q2_ref, kv_ref, k2_ref, out_ref, s_ref, dp_ref, m_ref, l_ref, d_ref, dq_ref, acc_ref):
    step = pl.program_id(0)
    count = LENGTH // BLOCK
    i = count - 1 - step

    @pl.when(step == 0)
    def _():
        acc_ref[...] = jnp.zeros_like(acc_ref)

    rows = pl.ds(pl.multiple_of(i * BLOCK, BLOCK), BLOCK)
    a = a_ref[rows, :]
    q2 = q2_ref[rows, :]
    lane = lax.broadcasted_iota(jnp.int32, (BLOCK, 128), 1)
    nope = jnp.where(lane < 64, a, jnp.zeros_like(a))
    cot = jnp.where(lane < 64, jnp.zeros_like(a), a)
    query = jnp.concatenate([nope, q2], axis=1)
    a_t = a.T
    q2_t = q2.T
    left_k = jnp.concatenate([q2_t[0:32], a_t[0:64]], axis=0)
    left_v = a_t[64:128]

    def tile(j):
        return pl.ds(pl.multiple_of(j * BLOCK, BLOCK), BLOCK)

    def key(j):
        return jnp.concatenate([kv_ref[tile(j), :], k2_ref[tile(j), :]], axis=1)

    m_ref[...] = jnp.full_like(m_ref, -1e30)
    l_ref[...] = jnp.zeros_like(l_ref)
    d_ref[...] = jnp.zeros_like(d_ref)
    dq_ref[...] = jnp.zeros_like(dq_ref)

    def scores(j, masked):
        s = dot_t(query, key(j))
        if masked:
            r = lax.broadcasted_iota(jnp.int32, (BLOCK, BLOCK), 0) // SPAN
            c = lax.broadcasted_iota(jnp.int32, (BLOCK, BLOCK), 1) // SPAN
            s = jnp.where(c <= r, s, -1e30)
        s_ref[:, tile(j)] = s
        m_ref[...] = jnp.maximum(m_ref[...], lanes(s, jnp.maximum))

    @pl.loop(0, i)
    def _(j):
        scores(j, False)

    scores(i, True)
    m = jnp.max(m_ref[...], axis=1, keepdims=True)

    def weights(j):
        dp = dot_t(cot, kv_ref[tile(j), :])
        e = jnp.exp2((s_ref[:, tile(j)] - m) * (SCALE * LOG2E))
        l_ref[...] += lanes(e, jnp.add)
        d_ref[...] += lanes(e * dp, jnp.add)
        s_ref[:, tile(j)] = e
        dp_ref[:, tile(j)] = dp

    @pl.loop(0, i + 1)
    def _(j):
        weights(j)

    inverse = 1.0 / jnp.sum(l_ref[...], axis=1, keepdims=True)
    delta = jnp.sum(d_ref[...], axis=1, keepdims=True) * inverse

    @pl.loop(0, i + 1)
    def _(j):
        p = s_ref[:, tile(j)] * inverse
        ds = (p * (dp_ref[:, tile(j)] - delta)).astype(bf16)
        dq_ref[...] += jnp.dot(ds, key(j), preferred_element_type=f32)
        acc_ref[0:96, tile(j)] += jnp.dot(left_k, ds, preferred_element_type=f32)
        acc_ref[96:160, tile(j)] += jnp.dot(left_v, p.astype(bf16), preferred_element_type=f32)

    dq = jnp.where(lane < 64, dq_ref[:, 0:128], pltpu.roll(dq_ref[:, 128:256], 64, 1)) * SCALE
    done = acc_ref[:, rows]
    k_rope = done[0:32] * SCALE
    k_nope = done[32:96] * SCALE
    low = jnp.concatenate([jnp.zeros((96, BLOCK), f32), k_rope], axis=0).T
    out_ref[:, 0:128] = jnp.where(lane < 96, dq, low).astype(bf16)
    out_ref[:, 128:256] = jnp.concatenate([k_nope, done[96:160]], axis=0).T.astype(bf16)


def attention(a, kv, ropes, head):
    count = LENGTH // BLOCK

    def column(k):
        return pl.BlockSpec((LENGTH, 128), lambda i: (0, k))

    return pl.pallas_call(
        attention_kernel,
        grid=(count,),
        in_specs=[column(2 * head), column(head), column(head), column(2)],
        out_specs=pl.BlockSpec((BLOCK, 256), lambda i: (count - 1 - i, 0)),
        out_shape=jax.ShapeDtypeStruct((LENGTH, 256), bf16),
        scratch_shapes=[
            pltpu.VMEM((BLOCK, LENGTH), f32),
            pltpu.VMEM((BLOCK, LENGTH), f32),
            pltpu.VMEM((BLOCK, 128), f32),
            pltpu.VMEM((BLOCK, 128), f32),
            pltpu.VMEM((BLOCK, 128), f32),
            pltpu.VMEM((BLOCK, 256), f32),
            pltpu.VMEM((160, LENGTH), f32),
        ],
        compiler_params=pltpu.CompilerParams(
            dimension_semantics=("arbitrary",), vmem_limit_bytes=48 * 1024 * 1024
        ),
        cost_estimate=pl.CostEstimate(
            flops=12_000_000_000, bytes_accessed=8_000_000, transcendentals=5_000_000
        ),
        name="attention",
    )(a, ropes, kv, ropes)


def finish_kernel(
    ret0, ret1, w, place, turn, latent, gain, cosine, sine,
    query_grad, latent_grad, rope_sum, acc,
):
    step = pl.program_id(0)

    @pl.when(step == 0)
    def _():
        acc[...] = jnp.zeros_like(acc)
        rope_sum[...] = jnp.zeros_like(rope_sum)

    left = [ret[t, :, 0:128] for t in range(2) for ret in (ret0, ret1)]
    row = jnp.concatenate(left, axis=1)
    plain = jnp.dot(row, place[...], preferred_element_type=f32)
    turned = jnp.dot(row, turn[...], preferred_element_type=f32)
    roped = lax.broadcasted_iota(jnp.int32, plain.shape, 1) % 96 >= 64
    wide_cos = jnp.where(roped, jnp.concatenate([cosine[...]] * 3, axis=1), 1.0)
    wide_sin = jnp.concatenate([sine[...]] * 3, axis=1)
    query_grad[...] = (plain * wide_cos + turned * wide_sin).astype(bf16)
    rope_sum[...] += sum(x.astype(f32) for x in left)
    total = acc[...]
    for t in range(2):
        right = jnp.concatenate([ret0[t, :, 128:256], ret1[t, :, 128:256]], axis=1)
        total += jnp.dot(right, w[t], preferred_element_type=f32)
    acc[...] = total

    @pl.when(step == pl.num_programs(0) - 1)
    def _():
        lat = latent[...].astype(f32)
        inverse = lax.rsqrt(jnp.mean(lat * lat, axis=1, keepdims=True) + eps)
        normed = lat * inverse
        scaled = acc[...] * gain[...]
        latent_grad[...] = inverse * (
            scaled - normed * jnp.mean(scaled * normed, axis=1, keepdims=True)
        )
        total_rope = rope_sum[...]
        rope_sum[...] = total_rope * cosine[...] - turned_halves(total_rope) * sine[...]


def finish(ret0, ret1, w, latent, gain, cosine, sine):
    fixed = lambda shape: pl.BlockSpec(shape, lambda j: (0,) * len(shape))
    place, turn = unpack_tables()
    return pl.pallas_call(
        finish_kernel,
        grid=(8,),
        in_specs=[
            pl.BlockSpec((2, TOKENS, 256), lambda j: (j, 0, 0)),
            pl.BlockSpec((2, TOKENS, 256), lambda j: (j, 0, 0)),
            pl.BlockSpec((2, 256, LATENT), lambda j: (j, 0, 0)),
            fixed((512, 384)),
            fixed((512, 384)),
            fixed((TOKENS, LATENT)),
            fixed((1, LATENT)),
            fixed((TOKENS, 128)),
            fixed((TOKENS, 128)),
        ],
        out_specs=[
            pl.BlockSpec((TOKENS, 384), lambda j: (0, j)),
            fixed((TOKENS, LATENT)),
            fixed((TOKENS, 128)),
        ],
        out_shape=[
            jax.ShapeDtypeStruct((TOKENS, 3072), bf16),
            jax.ShapeDtypeStruct((TOKENS, LATENT), f32),
            jax.ShapeDtypeStruct((TOKENS, 128), f32),
        ],
        scratch_shapes=[pltpu.VMEM((TOKENS, LATENT), f32)],
        compiler_params=pltpu.CompilerParams(dimension_semantics=("arbitrary",)),
        cost_estimate=pl.CostEstimate(
            flops=4_000_000_000, bytes_accessed=14_000_000, transcendentals=0
        ),
        name="finish",
    )(
        ret0, ret1, w, jnp.asarray(place, bf16), jnp.asarray(turn, bf16), latent, gain,
        cosine, sine,
    )


def inverse_frequency(index):
    return 1.0 / rope_base ** (2.0 * index.astype(f32) / ROPE)


def to_heads():
    pairs = []
    for i in range(DP_SIZE):
        for n in range(DP_SIZE):
            for b in range(2):
                pairs.append(((8 * b + n) * DP_SIZE + i, (2 * i + b) * DP_SIZE + n))
    return pairs


def place():
    z, y = lax.axis_index("sp_0"), lax.axis_index("sp_1")
    x, core = lax.axis_index("dp_0"), lax.axis_index("dp_1")
    return z, y, x, core


def on_sp(dz, dy):
    z, y, _, _ = place()
    return {"sp_0": lax.rem(z + dz, 4), "sp_1": lax.rem(y + dy, 4)}


def on_dp(dx, dcore):
    _, _, x, core = place()
    return {"dp_0": lax.rem(x + dx, 4), "dp_1": lax.rem(core + dcore, 2)}


SP_PEERS = [(k // 4, k % 4) for k in range(1, SP_SIZE)]
DP_PEERS = [(k // 2, k % 2) for k in range(1, DP_SIZE)]
MESSAGE_TURNS = [(4, 10, 9), (5, 13, 1), (6, 14), (3, 11), (2, 12), (7, 8), (0,), ()]
NEAR = [(0, 1), (0, 3), (1, 0), (3, 0)]
X_PEERS = [(1, 0), (3, 0), (0, 1)]


def meet(sp_peers, dp_peers):
    barrier = pltpu.get_barrier_semaphore()
    for where in [on_sp(*p) for p in sp_peers] + [on_dp(*p) for p in dp_peers]:
        pl.semaphore_signal(
            barrier, inc=1, device_id=where, device_id_type=pl.DeviceIdType.MESH
        )
    pl.semaphore_wait(barrier, len(sp_peers) + len(dp_peers))


def copy_to(src, dst, send, recv, where):
    c = pltpu.make_async_remote_copy(
        src_ref=src,
        dst_ref=dst,
        send_sem=send,
        recv_sem=recv,
        device_id=where,
        device_id_type=pl.DeviceIdType.MESH,
    )
    c.start()
    return c


def keep(src, dst, sem):
    c = pltpu.make_async_copy(src, dst, sem)
    c.start()
    return c


def send_over_sp(block_for, got, send, recv, chosen=range(SP_SIZE - 1)):
    z, y, _, _ = place()
    sent = []
    for k in chosen:
        dz, dy = SP_PEERS[k]
        there = 4 * lax.rem(z + dz, 4) + lax.rem(y + dy, 4)
        sent.append(
            copy_to(block_for(there), got.at[4 * z + y], send.at[k], recv.at[k], on_sp(dz, dy))
        )
    return sent


def send_over_dp(block_for, got, send, recv):
    _, _, x, core = place()
    sent = []
    for k, (dx, dcore) in enumerate(DP_PEERS):
        there = 2 * lax.rem(x + dx, 4) + lax.rem(core + dcore, 2)
        sent.append(
            copy_to(block_for(there), got.at[2 * x + core], send.at[k], recv.at[k], on_dp(dx, dcore))
        )
    return sent


def gather_over_sp(x, full, sems, between, midway=lambda: None):
    leg, leg_in, pass1, pass1_in, far, far_in, pass2, pass2_in = sems
    z, y, _, _ = place()
    me = 4 * z + y
    size = x.shape[0] // 2

    def along(h, s):
        return on_sp(0, s) if h == 0 else on_sp(s, 0)

    def across(h, s):
        return on_sp(s, 0) if h == 0 else on_sp(0, s)

    def block(h, s, c):
        dz, dy = (c, s) if h == 0 else (s, c)
        return 4 * lax.rem(z + dz, 4) + lax.rem(y + dy, 4)

    half = [pl.ds(h * size, size) for h in range(2)]
    quarter = [[pl.ds(h * size + q * size // 2, size // 2) for q in range(2)] for h in range(2)]
    ways = (1, 3)
    lines = (0, 3, 1, 2)
    first, second, third, fourth = {}, {}, {}, {}
    for w, s in enumerate(ways):
        for h in range(2):
            first[h, w] = copy_to(
                x.at[half[h]], full.at[me, half[h]], leg.at[h, w], leg_in.at[h, w], along(h, s)
            )
    for w, s in enumerate(ways):
        for h in range(2):
            third[h, 0, w] = copy_to(
                x.at[half[h]], full.at[me, half[h]], far.at[h, 0, w], far_in.at[h, 0, w], across(h, s)
            )
    rest = list(between(0))

    def onward(h, k):
        there = full.at[block(h, lines[k], 0), half[h]]
        for w, s in enumerate(ways):
            third[h, k, w] = copy_to(
                there, there, far.at[h, k, w], far_in.at[h, k, w], across(h, s)
            )

    for w, s in enumerate(ways):
        for h in range(2):
            first[h, w].wait_recv()
            piece = full.at[block(h, 4 - s, 0), quarter[h][w]]
            second[h, w] = copy_to(piece, piece, pass1.at[h, w], pass1_in.at[h, w], along(h, s))
            onward(h, w + 1)
        rest += between(w + 1)
    for h in range(2):
        for w in range(2):
            second[h, w].wait_recv()
        onward(h, 3)
    rest += between(3)
    for k in range(4):
        if k == 2:
            midway()
        for w, s in enumerate(ways):
            for h in range(2):
                third[h, k, w].wait_recv()
                piece = full.at[block(h, lines[k], 4 - s), quarter[h][w]]
                fourth[h, k, w] = copy_to(
                    piece, piece, pass2.at[h, k, w], pass2_in.at[h, k, w], across(h, s)
                )
        rest += between(k + 4)
    for group in (first, second, third):
        for c in group.values():
            c.wait_send()
    for c in list(fourth.values()) + rest:
        c.wait()


def front_kernel(x, msgs, w, full, got, w_full, own_sem, *sems):
    msg_send, msg_recv, ring, ring_in, pair, pair_in = sems[8:]
    z, y, chip, core = place()
    me = 4 * z + y
    mine = 2 * chip + core
    size = w.shape[0] // 2
    meet(SP_PEERS, X_PEERS)
    ways = (1, 3)
    beside = {}

    def to_partner(k, source, where):
        beside[k] = copy_to(source, w_full.at[where], pair.at[k], pair_in.at[k], on_dp(0, 1))

    out = [
        copy_to(w, w_full.at[mine], ring.at[0, k], ring_in.at[0, k], on_dp(s, 0))
        for k, s in enumerate(ways)
    ]
    to_partner(0, w, mine)

    def between(step):
        own = []
        if step == 0:
            own = [
                keep(x, full.at[me], own_sem.at[0]),
                keep(msgs.at[me], got.at[me], own_sem.at[1]),
                keep(w, w_full.at[mine], own_sem.at[2]),
            ]
        return own + send_over_sp(
            lambda there: msgs.at[there], got, msg_send, msg_recv, MESSAGE_TURNS[step]
        )

    def row(s):
        return 2 * lax.rem(chip + s, 4) + core

    passed = []

    def midway():
        for k, s in enumerate(ways):
            out[k].wait_recv()
            piece = w_full.at[row(4 - s), pl.ds(k * size, size)]
            passed.append(copy_to(piece, piece, ring.at[1, k], ring_in.at[1, k], on_dp(s, 0)))
            to_partner(1 + k, w_full.at[row(4 - s)], row(4 - s))

    gather_over_sp(x, full, sems[:8], between, midway)
    for c in passed:
        c.wait_recv()
    to_partner(3, w_full.at[row(2)], row(2))
    for c in out + passed:
        c.wait_send()
    for c in beside.values():
        c.wait()


def tail_kernel(msgs, pieces, gain, got, arrived, gains, own_sem, *sems):
    z, y, chip, core = place()
    me = 4 * z + y
    mine = 2 * chip + core
    meet(SP_PEERS, DP_PEERS)
    going = send_over_dp(lambda there: pieces.at[there], arrived, sems[0], sems[1])
    going += send_over_sp(lambda there: gain, gains, sems[2], sems[3])
    going += send_over_sp(lambda there: msgs.at[there], got, sems[4], sems[5])
    going.append(keep(pieces.at[mine], arrived.at[mine], own_sem.at[0]))
    going.append(keep(gain, gains.at[me], own_sem.at[1]))
    going.append(keep(msgs.at[me], got.at[me], own_sem.at[2]))
    for c in going:
        c.wait()


def last_kernel(x, gain, full, gains, own_sem, *sems):
    z, y, chip, core = place()
    meet(NEAR, DP_PEERS)

    def between(step):
        if step > 0:
            return []
        own = [
            keep(x, full.at[4 * z + y], own_sem.at[0]),
            keep(gain, gains.at[2 * chip + core], own_sem.at[1]),
        ]
        return own + send_over_dp(lambda there: gain, gains, sems[8], sems[9])

    gather_over_sp(x, full, sems[:8], between)


def moving(kernel, collective_id, operands, results, sem_shapes):
    dma = pltpu.SemaphoreType.DMA
    return pl.pallas_call(
        kernel,
        in_specs=[pl.BlockSpec(memory_space=pltpu.VMEM)] * len(operands),
        out_specs=[pl.BlockSpec(memory_space=pl.ANY)] * len(results),
        out_shape=[jax.ShapeDtypeStruct(shape, dtype) for shape, dtype in results],
        scratch_shapes=[dma((3,))] + [dma(shape) for shape in sem_shapes for _ in range(2)],
        compiler_params=pltpu.CompilerParams(collective_id=collective_id, has_side_effects=True),
        cost_estimate=pl.CostEstimate(
            flops=8_000_000_000, bytes_accessed=8_000_000, transcendentals=0
        ),
    )(*operands)


GATHER_SEMS = [(2, 2), (2, 2), (2, 4, 2), (2, 4, 2)]


def exchange(value):
    return lax.all_to_all(value, SP, split_axis=0, concat_axis=0, tiled=True)


def layer(query, latent, rope_key, latent_norm_gain, key_up_matrix, value_up_matrix, out_grad):
    lat = latent[0].astype(f32)
    inv_rms = lax.rsqrt(jnp.mean(lat * lat, axis=-1, keepdims=True) + eps)
    nlat = (lat * inv_rms * latent_norm_gain).astype(bf16)

    shard = jnp.stack(
        [key_up_matrix.reshape(2, 2, 64, LATENT), value_up_matrix.reshape(2, 2, 64, LATENT)],
        axis=2,
    ).reshape(2, 256, LATENT)
    spot = lax.axis_index(SP)
    half = lax.dynamic_index_in_dim(shard, spot // 8, 0, keepdims=False)
    w_own = lax.ppermute(half, SP_DP, to_heads())

    position = (spot * TOKENS + jnp.arange(TOKENS)).astype(f32)[:, None]
    angle = position * inverse_frequency(jnp.arange(128) % 16)[None]
    cosine, sine = jnp.cos(angle), jnp.sin(angle)
    rope_wide = jnp.pad(rope_key[0], ((0, 0), (0, 96)))
    sent = pack(query[0], out_grad[0], rope_wide, cosine, sine)
    nlat_full, got, w_whole = moving(
        front_kernel,
        0,
        [nlat, sent, shard.reshape(512, LATENT)],
        [
            ((SP_SIZE, TOKENS, LATENT), bf16),
            ((SP_SIZE, TOKENS, 384), bf16),
            ((DP_SIZE, 512, LATENT), bf16),
        ],
        GATHER_SEMS + [(SP_SIZE - 1,), (2, 2), (4,)],
    )
    nlat_full = nlat_full.reshape(LENGTH, LATENT)
    got = got.reshape(LENGTH, 384)
    w_whole = w_whole.reshape(SP_SIZE, 256, LATENT)

    ropes = jnp.dot(
        got[:, 128:256], jnp.asarray(rope_table(), bf16), preferred_element_type=f32
    ).astype(bf16)
    kv = lax.dot_general(
        nlat_full, w_own, (((1,), (1,)), ((), ())), preferred_element_type=f32
    ).astype(bf16)

    def weight_part(grads, h):
        d_w = lax.dot_general(
            grads[:, 128:256], nlat_full, (((0,), (0,)), ((), ())), preferred_element_type=f32
        )
        own = w_own[128 * h : 128 * h + 128].astype(f32)
        pieces = (
            d_w.reshape(2, DP_SIZE, 8, LATENT)
            .transpose(1, 0, 2, 3)
            .reshape(DP_SIZE, 16, LATENT)
        )
        return pieces, jnp.sum(d_w * own, axis=0)

    grads0 = attention(got, kv, ropes, 0)
    ret0 = exchange(grads0.reshape(SP_SIZE, TOKENS, 256))
    pieces0, gain0 = weight_part(grads0, 0)
    grads1 = attention(got, kv, ropes, 1)
    pieces1, gain1 = weight_part(grads1, 1)
    gain_part = ((gain0 + gain1) / latent_norm_gain).reshape(8, 128)
    ret1, arrived, gains = moving(
        tail_kernel,
        1,
        [
            grads1.reshape(SP_SIZE, TOKENS, 256),
            jnp.concatenate([pieces0, pieces1], axis=1),
            gain_part,
        ],
        [((SP_SIZE, TOKENS, 256), bf16), ((DP_SIZE, 32, LATENT), f32), ((SP_SIZE, 8, 128), f32)],
        [(DP_SIZE - 1,), (SP_SIZE - 1,), (SP_SIZE - 1,)],
    )
    moved = lax.ppermute(arrived.sum(axis=0), SP_DP, [(b, a) for a, b in to_heads()])
    blocks, gains = moving(
        last_kernel,
        2,
        [moved, gains.sum(axis=0)],
        [((SP_SIZE, 32, LATENT), f32), ((DP_SIZE, 8, 128), f32)],
        GATHER_SEMS + [(DP_SIZE - 1,)],
    )
    gain_grad = gains.sum(axis=0).reshape(LATENT)

    query_grad, latent_grad, rope_sum = finish(
        ret0, ret1, w_whole, latent[0], latent_norm_gain[None], cosine, sine
    )
    blocks = blocks.reshape(2, DP_SIZE, 2, 2, 8, LATENT).transpose(3, 0, 2, 1, 4, 5)
    blocks = blocks.reshape(2, 256, LATENT)
    return (
        query_grad[None],
        latent_grad[None],
        rope_sum[None, :, 96:128],
        blocks[0],
        blocks[1],
        gain_grad,
    )


def solution(mesh):
    split = Mesh(mesh.devices.reshape(4, 4, 4, 2), ("sp_0", "sp_1", "dp_0", "dp_1"))
    in_specs = (
        P(DP, SP, None),
        P(DP, SP, None),
        P(DP, SP, None),
        P(),
        P(DP, None),
        P(DP, None),
        P(DP, SP, None),
    )
    out_specs = (P(DP, SP, None), P(DP, SP, None), P(DP, SP, None), P(DP, None), P(DP, None), P())
    return jax.shard_map(layer, mesh=split, in_specs=in_specs, out_specs=out_specs, check_vma=False)
```

```python
import functools

import jax
import jax.numpy as jnp
import numpy as np
from jax import lax
from jax.experimental import pallas as pl
from jax.experimental.pallas import tpu as pltpu
from jax.sharding import Mesh
from jax.sharding import PartitionSpec as P


PLAIN_HEAD_WIDTH = 64
ROPE = 32
SPAN = 64
LATENT = 1024
LENGTH = 3072
TOKENS = 192
DP = ("dp_0", "dp_1")
SP = ("sp_0", "sp_1")
SP_DP = ("sp_0", "sp_1", "dp_0", "dp_1")
SP_SIZE = 16
DP_SIZE = 8
BLOCK = 512
SCALE = (PLAIN_HEAD_WIDTH + ROPE) ** (-0.5)
LOG2E = 1.4426950408889634

eps = 1e-06
rope_base = 10000.0
f32 = jnp.float32
bf16 = jnp.bfloat16


def pack_tables():
    first = np.zeros((384 + 256 + 128, 512), np.float32)
    second = np.zeros((384 + 256 + 128, 256), np.float32)
    for t in range(2):
        q, d, r = 192 * t, 384 + 128 * t, 640
        for c in range(64):
            first[q + c, 256 * t + c] = 1
            first[d + c, 256 * t + 64 + c] = 1
            second[q + 96 + c, 128 * t + c] = 1
            second[d + 64 + c, 128 * t + 64 + c] = 1
        for c in range(32):
            first[q + 64 + c, 256 * t + 128 + c] = 1
            first[q + 160 + c, 256 * t + 160 + c] = 1
            first[r + c, 256 * t + 192 + c] = 1
    return first, second


def unpack_tables():
    place = np.zeros((512, 384), np.float32)
    turn = np.zeros((512, 384), np.float32)
    for t in range(2):
        for h in range(2):
            row, col = 256 * t + 128 * h, 192 * t + 96 * h
            for c in range(96):
                place[row + c, col + c] = 1
            for c in range(64, 80):
                turn[row + c + 16, col + c] = 1
                turn[row + c, col + c + 16] = -1
    return place, turn


def rope_table():
    spread = np.zeros((128, 384), np.float32)
    for c in range(32):
        spread[c, c] = 1
        spread[32 + c, 128 + c] = 1
        spread[64 + c, 256 + c] = 1
    return spread


def turned_halves(x):
    lane = lax.broadcasted_iota(jnp.int32, x.shape, 1)
    return jnp.where(lane % 32 < 16, -pltpu.roll(x, 112, 1), pltpu.roll(x, 16, 1))


def pack_kernel(query, d_out, rope, first, second, cosine, sine, out):
    both = jnp.concatenate([query[...], d_out[...], rope[...]], axis=1)
    one = jnp.dot(both, first[...], preferred_element_type=f32)
    two = jnp.dot(both, second[...], preferred_element_type=f32).astype(bf16)
    for t in range(2):
        out[t, :, 0:128] = one[:, 256 * t : 256 * t + 128].astype(bf16)
        raw = one[:, 256 * t + 128 : 256 * t + 256]
        out[t, :, 128:256] = (raw * cosine[...] + turned_halves(raw) * sine[...]).astype(bf16)
        out[t, :, 256:384] = two[:, 128 * t : 128 * t + 128]


def pack(query, d_out, rope, cosine, sine):
    first, second = pack_tables()
    whole = lambda shape: pl.BlockSpec(shape, lambda j: (0, 0))
    return pl.pallas_call(
        pack_kernel,
        grid=(8,),
        in_specs=[
            pl.BlockSpec((TOKENS, 384), lambda j: (0, j)),
            pl.BlockSpec((TOKENS, 256), lambda j: (0, j)),
            whole((TOKENS, 128)),
            whole((768, 512)),
            whole((768, 256)),
            whole((TOKENS, 128)),
            whole((TOKENS, 128)),
        ],
        out_specs=pl.BlockSpec((2, TOKENS, 384), lambda j: (j, 0, 0)),
        out_shape=jax.ShapeDtypeStruct((SP_SIZE, TOKENS, 384), bf16),
        cost_estimate=pl.CostEstimate(
            flops=16 * 192 * 768 * 768, bytes_accessed=5_000_000, transcendentals=0
        ),
        name="pack",
    )(query, d_out, rope, jnp.asarray(first, bf16), jnp.asarray(second, bf16), cosine, sine)


def dot_t(a, b):
    return lax.dot_general(a, b, (((1,), (1,)), ((), ())), preferred_element_type=f32)


def lanes(x, combine):
    parts = [x[:, k : k + 128] for k in range(0, x.shape[1], 128)]
    return functools.reduce(combine, parts)


def attention_kernel(a_ref, q2_ref, kv_ref, k2_ref, out_ref, s_ref, dp_ref, m_ref, l_ref, d_ref, dq_ref, acc_ref):
    step = pl.program_id(0)
    count = LENGTH // BLOCK
    i = count - 1 - step

    @pl.when(step == 0)
    def _():
        acc_ref[...] = jnp.zeros_like(acc_ref)

    rows = pl.ds(pl.multiple_of(i * BLOCK, BLOCK), BLOCK)
    a = a_ref[rows, :]
    q2 = q2_ref[rows, :]
    lane = lax.broadcasted_iota(jnp.int32, (BLOCK, 128), 1)
    nope = jnp.where(lane < 64, a, jnp.zeros_like(a))
    cot = jnp.where(lane < 64, jnp.zeros_like(a), a)
    query = jnp.concatenate([nope, q2], axis=1)
    a_t = a.T
    q2_t = q2.T
    left_k = jnp.concatenate([q2_t[0:32], a_t[0:64]], axis=0)
    left_v = a_t[64:128]

    def tile(j):
        return pl.ds(pl.multiple_of(j * BLOCK, BLOCK), BLOCK)

    def key(j):
        return jnp.concatenate([kv_ref[tile(j), :], k2_ref[tile(j), :]], axis=1)

    m_ref[...] = jnp.full_like(m_ref, -1e30)
    l_ref[...] = jnp.zeros_like(l_ref)
    d_ref[...] = jnp.zeros_like(d_ref)
    dq_ref[...] = jnp.zeros_like(dq_ref)

    def scores(j, masked):
        s = dot_t(query, key(j))
        if masked:
            r = lax.broadcasted_iota(jnp.int32, (BLOCK, BLOCK), 0) // SPAN
            c = lax.broadcasted_iota(jnp.int32, (BLOCK, BLOCK), 1) // SPAN
            s = jnp.where(c <= r, s, -1e30)
        s_ref[:, tile(j)] = s
        m_ref[...] = jnp.maximum(m_ref[...], lanes(s, jnp.maximum))

    @pl.loop(0, i)
    def _(j):
        scores(j, False)

    scores(i, True)
    m = jnp.max(m_ref[...], axis=1, keepdims=True)

    def weights(j):
        dp = dot_t(cot, kv_ref[tile(j), :])
        e = jnp.exp2((s_ref[:, tile(j)] - m) * (SCALE * LOG2E))
        l_ref[...] += lanes(e, jnp.add)
        d_ref[...] += lanes(e * dp, jnp.add)
        s_ref[:, tile(j)] = e
        dp_ref[:, tile(j)] = dp

    @pl.loop(0, i + 1)
    def _(j):
        weights(j)

    inverse = 1.0 / jnp.sum(l_ref[...], axis=1, keepdims=True)
    delta = jnp.sum(d_ref[...], axis=1, keepdims=True) * inverse

    @pl.loop(0, i + 1)
    def _(j):
        p = s_ref[:, tile(j)] * inverse
        ds = (p * (dp_ref[:, tile(j)] - delta)).astype(bf16)
        dq_ref[...] += jnp.dot(ds, key(j), preferred_element_type=f32)
        acc_ref[0:96, tile(j)] += jnp.dot(left_k, ds, preferred_element_type=f32)
        acc_ref[96:160, tile(j)] += jnp.dot(left_v, p.astype(bf16), preferred_element_type=f32)

    dq = jnp.where(lane < 64, dq_ref[:, 0:128], pltpu.roll(dq_ref[:, 128:256], 64, 1)) * SCALE
    done = acc_ref[:, rows]
    k_rope = done[0:32] * SCALE
    k_nope = done[32:96] * SCALE
    low = jnp.concatenate([jnp.zeros((96, BLOCK), f32), k_rope], axis=0).T
    out_ref[:, 0:128] = jnp.where(lane < 96, dq, low).astype(bf16)
    out_ref[:, 128:256] = jnp.concatenate([k_nope, done[96:160]], axis=0).T.astype(bf16)


def attention(a, kv, ropes, head):
    count = LENGTH // BLOCK

    def column(k):
        return pl.BlockSpec((LENGTH, 128), lambda i: (0, k))

    return pl.pallas_call(
        attention_kernel,
        grid=(count,),
        in_specs=[column(2 * head), column(head), column(head), column(2)],
        out_specs=pl.BlockSpec((BLOCK, 256), lambda i: (count - 1 - i, 0)),
        out_shape=jax.ShapeDtypeStruct((LENGTH, 256), bf16),
        scratch_shapes=[
            pltpu.VMEM((BLOCK, LENGTH), f32),
            pltpu.VMEM((BLOCK, LENGTH), f32),
            pltpu.VMEM((BLOCK, 128), f32),
            pltpu.VMEM((BLOCK, 128), f32),
            pltpu.VMEM((BLOCK, 128), f32),
            pltpu.VMEM((BLOCK, 256), f32),
            pltpu.VMEM((160, LENGTH), f32),
        ],
        compiler_params=pltpu.CompilerParams(
            dimension_semantics=("arbitrary",), vmem_limit_bytes=48 * 1024 * 1024
        ),
        cost_estimate=pl.CostEstimate(
            flops=12_000_000_000, bytes_accessed=8_000_000, transcendentals=5_000_000
        ),
        name="attention",
    )(a, ropes, kv, ropes)


def finish_kernel(
    ret0, ret1, w, place, turn, latent, gain, cosine, sine,
    query_grad, latent_grad, rope_sum, acc,
):
    step = pl.program_id(0)

    @pl.when(step == 0)
    def _():
        acc[...] = jnp.zeros_like(acc)
        rope_sum[...] = jnp.zeros_like(rope_sum)

    left = [ret[t, :, 0:128] for t in range(2) for ret in (ret0, ret1)]
    row = jnp.concatenate(left, axis=1)
    plain = jnp.dot(row, place[...], preferred_element_type=f32)
    turned = jnp.dot(row, turn[...], preferred_element_type=f32)
    roped = lax.broadcasted_iota(jnp.int32, plain.shape, 1) % 96 >= 64
    wide_cos = jnp.where(roped, jnp.concatenate([cosine[...]] * 3, axis=1), 1.0)
    wide_sin = jnp.concatenate([sine[...]] * 3, axis=1)
    query_grad[...] = (plain * wide_cos + turned * wide_sin).astype(bf16)
    rope_sum[...] += sum(x.astype(f32) for x in left)
    total = acc[...]
    for t in range(2):
        right = jnp.concatenate([ret0[t, :, 128:256], ret1[t, :, 128:256]], axis=1)
        total += jnp.dot(right, w[t], preferred_element_type=f32)
    acc[...] = total

    @pl.when(step == pl.num_programs(0) - 1)
    def _():
        lat = latent[...].astype(f32)
        inverse = lax.rsqrt(jnp.mean(lat * lat, axis=1, keepdims=True) + eps)
        normed = lat * inverse
        scaled = acc[...] * gain[...]
        latent_grad[...] = inverse * (
            scaled - normed * jnp.mean(scaled * normed, axis=1, keepdims=True)
        )
        total_rope = rope_sum[...]
        rope_sum[...] = total_rope * cosine[...] - turned_halves(total_rope) * sine[...]


def finish(ret0, ret1, w, latent, gain, cosine, sine):
    fixed = lambda shape: pl.BlockSpec(shape, lambda j: (0,) * len(shape))
    place, turn = unpack_tables()
    return pl.pallas_call(
        finish_kernel,
        grid=(8,),
        in_specs=[
            pl.BlockSpec((2, TOKENS, 256), lambda j: (j, 0, 0)),
            pl.BlockSpec((2, TOKENS, 256), lambda j: (j, 0, 0)),
            pl.BlockSpec((2, 256, LATENT), lambda j: (j, 0, 0)),
            fixed((512, 384)),
            fixed((512, 384)),
            fixed((TOKENS, LATENT)),
            fixed((1, LATENT)),
            fixed((TOKENS, 128)),
            fixed((TOKENS, 128)),
        ],
        out_specs=[
            pl.BlockSpec((TOKENS, 384), lambda j: (0, j)),
            fixed((TOKENS, LATENT)),
            fixed((TOKENS, 128)),
        ],
        out_shape=[
            jax.ShapeDtypeStruct((TOKENS, 3072), bf16),
            jax.ShapeDtypeStruct((TOKENS, LATENT), f32),
            jax.ShapeDtypeStruct((TOKENS, 128), f32),
        ],
        scratch_shapes=[pltpu.VMEM((TOKENS, LATENT), f32)],
        compiler_params=pltpu.CompilerParams(dimension_semantics=("arbitrary",)),
        cost_estimate=pl.CostEstimate(
            flops=4_000_000_000, bytes_accessed=14_000_000, transcendentals=0
        ),
        name="finish",
    )(
        ret0, ret1, w, jnp.asarray(place, bf16), jnp.asarray(turn, bf16), latent, gain,
        cosine, sine,
    )


def inverse_frequency(index):
    return 1.0 / rope_base ** (2.0 * index.astype(f32) / ROPE)


def to_heads():
    pairs = []
    for i in range(DP_SIZE):
        for n in range(DP_SIZE):
            for b in range(2):
                pairs.append(((8 * b + n) * DP_SIZE + i, (2 * i + b) * DP_SIZE + n))
    return pairs


def place():
    z, y = lax.axis_index("sp_0"), lax.axis_index("sp_1")
    x, core = lax.axis_index("dp_0"), lax.axis_index("dp_1")
    return z, y, x, core


def on_sp(dz, dy):
    z, y, _, _ = place()
    return {"sp_0": lax.rem(z + dz, 4), "sp_1": lax.rem(y + dy, 4)}


def on_dp(dx, dcore):
    _, _, x, core = place()
    return {"dp_0": lax.rem(x + dx, 4), "dp_1": lax.rem(core + dcore, 2)}


SP_PEERS = [(k // 4, k % 4) for k in range(1, SP_SIZE)]
DP_PEERS = [(k // 2, k % 2) for k in range(1, DP_SIZE)]
MESSAGE_TURNS = [(4, 10, 9), (5, 13, 1), (6, 14), (3, 11), (2, 12), (7, 8), (0,), ()]
NEAR = [(0, 1), (0, 3), (1, 0), (3, 0)]
X_PEERS = [(1, 0), (3, 0), (0, 1)]


def meet(sp_peers, dp_peers):
    barrier = pltpu.get_barrier_semaphore()
    for where in [on_sp(*p) for p in sp_peers] + [on_dp(*p) for p in dp_peers]:
        pl.semaphore_signal(
            barrier, inc=1, device_id=where, device_id_type=pl.DeviceIdType.MESH
        )
    pl.semaphore_wait(barrier, len(sp_peers) + len(dp_peers))


def copy_to(src, dst, send, recv, where):
    c = pltpu.make_async_remote_copy(
        src_ref=src,
        dst_ref=dst,
        send_sem=send,
        recv_sem=recv,
        device_id=where,
        device_id_type=pl.DeviceIdType.MESH,
    )
    c.start()
    return c


def keep(src, dst, sem):
    c = pltpu.make_async_copy(src, dst, sem)
    c.start()
    return c


def send_over_sp(block_for, got, send, recv, chosen=range(SP_SIZE - 1)):
    z, y, _, _ = place()
    sent = []
    for k in chosen:
        dz, dy = SP_PEERS[k]
        there = 4 * lax.rem(z + dz, 4) + lax.rem(y + dy, 4)
        sent.append(
            copy_to(block_for(there), got.at[4 * z + y], send.at[k], recv.at[k], on_sp(dz, dy))
        )
    return sent


def send_over_dp(block_for, got, send, recv):
    _, _, x, core = place()
    sent = []
    for k, (dx, dcore) in enumerate(DP_PEERS):
        there = 2 * lax.rem(x + dx, 4) + lax.rem(core + dcore, 2)
        sent.append(
            copy_to(block_for(there), got.at[2 * x + core], send.at[k], recv.at[k], on_dp(dx, dcore))
        )
    return sent


def gather_over_sp(x, full, sems, between, midway=lambda k: None):
    leg, leg_in, pass1, pass1_in, far, far_in, pass2, pass2_in = sems
    z, y, _, _ = place()
    me = 4 * z + y
    size = x.shape[0] // 2

    def along(h, s):
        return on_sp(0, s) if h == 0 else on_sp(s, 0)

    def across(h, s):
        return on_sp(s, 0) if h == 0 else on_sp(0, s)

    def block(h, s, c):
        dz, dy = (c, s) if h == 0 else (s, c)
        return 4 * lax.rem(z + dz, 4) + lax.rem(y + dy, 4)

    half = [pl.ds(h * size, size) for h in range(2)]
    quarter = [[pl.ds(h * size + q * size // 2, size // 2) for q in range(2)] for h in range(2)]
    ways = (1, 3)
    lines = (0, 3, 1, 2)
    first, second, third, fourth = {}, {}, {}, {}
    for w, s in enumerate(ways):
        for h in range(2):
            first[h, w] = copy_to(
                x.at[half[h]], full.at[me, half[h]], leg.at[h, w], leg_in.at[h, w], along(h, s)
            )
    for w, s in enumerate(ways):
        for h in range(2):
            third[h, 0, w] = copy_to(
                x.at[half[h]], full.at[me, half[h]], far.at[h, 0, w], far_in.at[h, 0, w], across(h, s)
            )
    rest = list(between(0))

    def onward(h, k):
        there = full.at[block(h, lines[k], 0), half[h]]
        for w, s in enumerate(ways):
            third[h, k, w] = copy_to(
                there, there, far.at[h, k, w], far_in.at[h, k, w], across(h, s)
            )

    for w, s in enumerate(ways):
        for h in range(2):
            first[h, w].wait_recv()
            piece = full.at[block(h, 4 - s, 0), quarter[h][w]]
            second[h, w] = copy_to(piece, piece, pass1.at[h, w], pass1_in.at[h, w], along(h, s))
            onward(h, w + 1)
        rest += between(w + 1)
    for h in range(2):
        for w in range(2):
            second[h, w].wait_recv()
        onward(h, 3)
    rest += between(3)
    for k in range(4):
        midway(k)
        for w, s in enumerate(ways):
            for h in range(2):
                third[h, k, w].wait_recv()
                piece = full.at[block(h, lines[k], 4 - s), quarter[h][w]]
                fourth[h, k, w] = copy_to(
                    piece, piece, pass2.at[h, k, w], pass2_in.at[h, k, w], across(h, s)
                )
        rest += between(k + 4)
    for group in (first, second, third):
        for c in group.values():
            c.wait_send()
    for c in list(fourth.values()) + rest:
        c.wait()


def front_kernel(x, msgs, w, full, got, w_full, own_sem, *sems):
    msg_send, msg_recv, ring, ring_in, pair, pair_in = sems[8:]
    z, y, chip, core = place()
    me = 4 * z + y
    mine = 2 * chip + core
    size = w.shape[0] // 2
    meet(SP_PEERS, X_PEERS)
    ways = (1, 3)
    beside = {}

    def to_partner(k, source, where):
        beside[k] = copy_to(source, w_full.at[where], pair.at[k], pair_in.at[k], on_dp(0, 1))

    out = [
        copy_to(w, w_full.at[mine], ring.at[0, k], ring_in.at[0, k], on_dp(s, 0))
        for k, s in enumerate(ways)
    ]
    to_partner(0, w, mine)

    def between(step):
        own = []
        if step == 0:
            own = [
                keep(x, full.at[me], own_sem.at[0]),
                keep(msgs.at[me], got.at[me], own_sem.at[1]),
                keep(w, w_full.at[mine], own_sem.at[2]),
            ]
        return own + send_over_sp(
            lambda there: msgs.at[there], got, msg_send, msg_recv, MESSAGE_TURNS[step]
        )

    def row(s):
        return 2 * lax.rem(chip + s, 4) + core

    passed = []

    def midway(step):
        if step == 0:
            for k, s in enumerate(ways):
                out[k].wait_recv()
                piece = w_full.at[row(4 - s), pl.ds(k * size, size)]
                passed.append(copy_to(piece, piece, ring.at[1, k], ring_in.at[1, k], on_dp(s, 0)))
                to_partner(1 + k, w_full.at[row(4 - s)], row(4 - s))
        if step == 3:
            for c in passed:
                c.wait_recv()
            to_partner(3, w_full.at[row(2)], row(2))

    gather_over_sp(x, full, sems[:8], between, midway)
    for c in out + passed:
        c.wait_send()
    for c in beside.values():
        c.wait()


def tail_kernel(msgs, pieces, gain, got, arrived, gains, own_sem, *sems):
    z, y, chip, core = place()
    me = 4 * z + y
    mine = 2 * chip + core
    meet(SP_PEERS, DP_PEERS)
    going = send_over_dp(lambda there: pieces.at[there], arrived, sems[0], sems[1])
    going += send_over_sp(lambda there: gain, gains, sems[2], sems[3])
    going += send_over_sp(lambda there: msgs.at[there], got, sems[4], sems[5])
    going.append(keep(pieces.at[mine], arrived.at[mine], own_sem.at[0]))
    going.append(keep(gain, gains.at[me], own_sem.at[1]))
    going.append(keep(msgs.at[me], got.at[me], own_sem.at[2]))
    for c in going:
        c.wait()


def last_kernel(x, gain, full, gains, own_sem, *sems):
    z, y, chip, core = place()
    meet(NEAR, DP_PEERS)

    def between(step):
        if step > 0:
            return []
        own = [
            keep(x, full.at[4 * z + y], own_sem.at[0]),
            keep(gain, gains.at[2 * chip + core], own_sem.at[1]),
        ]
        return own + send_over_dp(lambda there: gain, gains, sems[8], sems[9])

    gather_over_sp(x, full, sems[:8], between)


def moving(kernel, collective_id, operands, results, sem_shapes):
    dma = pltpu.SemaphoreType.DMA
    return pl.pallas_call(
        kernel,
        in_specs=[pl.BlockSpec(memory_space=pltpu.VMEM)] * len(operands),
        out_specs=[pl.BlockSpec(memory_space=pl.ANY)] * len(results),
        out_shape=[jax.ShapeDtypeStruct(shape, dtype) for shape, dtype in results],
        scratch_shapes=[dma((3,))] + [dma(shape) for shape in sem_shapes for _ in range(2)],
        compiler_params=pltpu.CompilerParams(collective_id=collective_id, has_side_effects=True),
        cost_estimate=pl.CostEstimate(
            flops=8_000_000_000, bytes_accessed=8_000_000, transcendentals=0
        ),
    )(*operands)


GATHER_SEMS = [(2, 2), (2, 2), (2, 4, 2), (2, 4, 2)]


def exchange(value):
    return lax.all_to_all(value, SP, split_axis=0, concat_axis=0, tiled=True)


def layer(query, latent, rope_key, latent_norm_gain, key_up_matrix, value_up_matrix, out_grad):
    lat = latent[0].astype(f32)
    inv_rms = lax.rsqrt(jnp.mean(lat * lat, axis=-1, keepdims=True) + eps)
    nlat = (lat * inv_rms * latent_norm_gain).astype(bf16)

    shard = jnp.stack(
        [key_up_matrix.reshape(2, 2, 64, LATENT), value_up_matrix.reshape(2, 2, 64, LATENT)],
        axis=2,
    ).reshape(2, 256, LATENT)
    spot = lax.axis_index(SP)
    half = lax.dynamic_index_in_dim(shard, spot // 8, 0, keepdims=False)
    w_own = lax.ppermute(half, SP_DP, to_heads())

    position = (spot * TOKENS + jnp.arange(TOKENS)).astype(f32)[:, None]
    angle = position * inverse_frequency(jnp.arange(128) % 16)[None]
    cosine, sine = jnp.cos(angle), jnp.sin(angle)
    rope_wide = jnp.pad(rope_key[0], ((0, 0), (0, 96)))
    sent = pack(query[0], out_grad[0], rope_wide, cosine, sine)
    nlat_full, got, w_whole = moving(
        front_kernel,
        0,
        [nlat, sent, shard.reshape(512, LATENT)],
        [
            ((SP_SIZE, TOKENS, LATENT), bf16),
            ((SP_SIZE, TOKENS, 384), bf16),
            ((DP_SIZE, 512, LATENT), bf16),
        ],
        GATHER_SEMS + [(SP_SIZE - 1,), (2, 2), (4,)],
    )
    nlat_full = nlat_full.reshape(LENGTH, LATENT)
    got = got.reshape(LENGTH, 384)
    w_whole = w_whole.reshape(SP_SIZE, 256, LATENT)

    ropes = jnp.dot(
        got[:, 128:256], jnp.asarray(rope_table(), bf16), preferred_element_type=f32
    ).astype(bf16)
    kv = lax.dot_general(
        nlat_full, w_own, (((1,), (1,)), ((), ())), preferred_element_type=f32
    ).astype(bf16)

    def weight_part(grads, h):
        d_w = lax.dot_general(
            grads[:, 128:256], nlat_full, (((0,), (0,)), ((), ())), preferred_element_type=f32
        )
        own = w_own[128 * h : 128 * h + 128].astype(f32)
        pieces = (
            d_w.reshape(2, DP_SIZE, 8, LATENT)
            .transpose(1, 0, 2, 3)
            .reshape(DP_SIZE, 16, LATENT)
        )
        return pieces, jnp.sum(d_w * own, axis=0)

    grads0 = attention(got, kv, ropes, 0)
    ret0 = exchange(grads0.reshape(SP_SIZE, TOKENS, 256))
    pieces0, gain0 = weight_part(grads0, 0)
    grads1 = attention(got, kv, ropes, 1)
    pieces1, gain1 = weight_part(grads1, 1)
    gain_part = ((gain0 + gain1) / latent_norm_gain).reshape(8, 128)
    ret1, arrived, gains = moving(
        tail_kernel,
        1,
        [
            grads1.reshape(SP_SIZE, TOKENS, 256),
            jnp.concatenate([pieces0, pieces1], axis=1),
            gain_part,
        ],
        [((SP_SIZE, TOKENS, 256), bf16), ((DP_SIZE, 32, LATENT), f32), ((SP_SIZE, 8, 128), f32)],
        [(DP_SIZE - 1,), (SP_SIZE - 1,), (SP_SIZE - 1,)],
    )
    moved = lax.ppermute(arrived.sum(axis=0).astype(bf16), SP_DP, [(b, a) for a, b in to_heads()])
    blocks, gains = moving(
        last_kernel,
        2,
        [moved, gains.sum(axis=0)],
        [((SP_SIZE, 32, LATENT), bf16), ((DP_SIZE, 8, 128), f32)],
        GATHER_SEMS + [(DP_SIZE - 1,)],
    )
    gain_grad = gains.sum(axis=0).reshape(LATENT)

    query_grad, latent_grad, rope_sum = finish(
        ret0, ret1, w_whole, latent[0], latent_norm_gain[None], cosine, sine
    )
    blocks = blocks.reshape(2, DP_SIZE, 2, 2, 8, LATENT).transpose(3, 0, 2, 1, 4, 5)
    blocks = blocks.reshape(2, 256, LATENT).astype(f32)
    return (
        query_grad[None],
        latent_grad[None],
        rope_sum[None, :, 96:128],
        blocks[0],
        blocks[1],
        gain_grad,
    )


def solution(mesh):
    split = Mesh(mesh.devices.reshape(4, 4, 4, 2), ("sp_0", "sp_1", "dp_0", "dp_1"))
    in_specs = (
        P(DP, SP, None),
        P(DP, SP, None),
        P(DP, SP, None),
        P(),
        P(DP, None),
        P(DP, None),
        P(DP, SP, None),
    )
    out_specs = (P(DP, SP, None), P(DP, SP, None), P(DP, SP, None), P(DP, None), P(DP, None), P())
    return jax.shard_map(layer, mesh=split, in_specs=in_specs, out_specs=out_specs, check_vma=False)
```
